512 devices in a mesh: ep: 128 (over z, x, core), tp: 4 (over y).
Axes of the slice: x: 4, y: 4, z: 16, core: 2. Of those that a mesh axis runs over, the one named last changes fastest.
Arguments:
- residual_in: bfloat16 [1920, 1536], P('ep'), may hold values from -6 to 6
- rec_state: bfloat16 [1920, 12, 128, 128], P('ep', 'tp'), may hold values from -6 to 6
- mix_gain: float32 [1536], replicated, may hold values from 0.1 to 1.9
- w_query: bfloat16 [1536, 1536], P('tp', 'ep'), may hold values from -0.15625 to 0.15625
- w_forget: bfloat16 [1536, 1536], P('tp', 'ep'), may hold values from -0.15625 to 0.15625
- w_input: bfloat16 [1536, 1536], P('tp', 'ep'), may hold values from -0.15625 to 0.15625
- w_gate: bfloat16 [1536, 1536], P('tp', 'ep'), may hold values from -0.15625 to 0.15625
- lower_bound: float32 [1536], P('tp'), may hold values from 0 to 0.9
- head_gain: float32 [128], replicated, may hold values from 0.1 to 1.9
- w_out: bfloat16 [1536, 1536], P('tp', 'ep'), may hold values from -0.15625 to 0.15625
- ffn_gain: float32 [1536], replicated, may hold values from 0.1 to 1.9
- route_ids: int32 [1920, 6], P('ep'), may hold values from 0 to 127, all different within a row; in each aligned block of 15 rows (0 to 14, 15 to 29, ...) at most 2 rows name the same one
- route_weight: float32 [1920, 6], P('ep'), may hold values from 0.2 to 1
- expert_gate: bfloat16 [128, 1536, 512], P('ep', None, 'tp'), may hold values from -0.15625 to 0.15625
- expert_up: bfloat16 [128, 1536, 512], P('ep', None, 'tp'), may hold values from -0.15625 to 0.15625
- expert_down: bfloat16 [128, 512, 1536], P('ep', 'tp'), may hold values from -0.25 to 0.25
Outputs:
- layer_out: bfloat16 [1920, 1536], P('ep', 'tp')
- new_state: bfloat16 [1920, 12, 128, 128], P('ep', 'tp')
The draws below stay inside these ranges and needn't reach their ends.
Inputs may be any that keep to these rules, and one draw needn't show every extreme that they name: `route_ids`: each row names 6 different experts. Among the rows of one device no expert is named more than 2 times, and in every draw some device names some expert exactly 2 times.
All inputs are finite; a program needn't handle non-finite values.
Results may differ from the reference program's by a relative error of at most 0.016.
Values may be sent and summed in bfloat16 or wider, within the bound.
A program may use at most 64 MiB of HBM per device.

```python
import math
import jax
import jax.numpy as jnp
import numpy as np
from jax import lax

D = 1536
HEADS = 12
FF = 512
TOPK = 6
SEQ_DEV = 15
HEAD = 128
TOKENS = 1920
EXPERTS = 128
CAP = 2
N_EP = 128


def level_of(rng, dims, split, least, largest):
    level, own = 1.0, jax.random.fold_in(rng, 6)
    for position, shards_of in split:
        draws = jnp.exp(jax.random.uniform(jax.random.fold_in(own, position), (shards_of,), jnp.float32, least / len(split), largest / len(split)))
        level = level * jnp.repeat(draws, dims[position] // shards_of).reshape([-1 if axis == position else 1 for axis in range(len(dims))])
    return level


def shared_out(rng, own, number, rows, amount, top, bound, slope):
    ranking = jax.random.permutation(rng, amount)
    crowded, usual = shares(amount, rows * top, bound, slope, True), shares(amount, rows * top, bound, slope, False)
    places = jnp.arange(amount)

    def named(tallies, offset_by):
        used = int((tallies > 0).sum())
        fixed = max(1, used // 4)
        shifted = fixed + (places - fixed + offset_by * (used - fixed)) % max(1, amount - fixed)
        return jnp.zeros((amount,), jnp.int32).at[ranking[jnp.where(places < fixed, places, shifted)]].set(jnp.asarray(tallies, jnp.int32))

    tallies = jnp.where(number % 4 == 0, named(crowded, number // 4), named(usual, number - number // 4 - 1))
    mixed = jax.random.permutation(jax.random.fold_in(own, 3), amount)
    giver, sink = mixed[0:amount // 2 * 2:2], mixed[1:amount // 2 * 2:2]
    slack = jnp.minimum(tallies[giver] - 1, bound - tallies[sink]) // 2
    slack = jnp.where((giver == ranking[0]) | (sink == ranking[0]) | (tallies[sink] == 0), 0, jnp.maximum(slack, 0))
    shifted = jax.random.randint(jax.random.fold_in(own, 4), (amount // 2,), 0, 1 << 20) % (slack + 1)
    tallies = tallies.at[giver].add(-shifted).at[sink].add(shifted)
    members = jnp.searchsorted(jnp.cumsum(tallies), jnp.arange(rows * top), side="right").astype(jnp.int32)
    listing = members.reshape(top, rows).T
    listing = listing[jax.random.permutation(jax.random.fold_in(own, 1), rows)]
    offset_by = jax.random.randint(jax.random.fold_in(own, 2), (rows, 1), 0, top)
    return jnp.take_along_axis(listing, (jnp.arange(top)[None, :] + offset_by) % top, axis=1)


def shares(count, total, reach, lean, full):
    loads = [(1 << 20) // math.isqrt(rank ** lean) + 1 for rank in range(1, count + 1)]
    largest = reach if full else min(reach, max(-(-total // count), total * loads[0] // sum(loads)))
    least = 1 if total - largest >= count - 1 else 0
    given, rest = [largest] + [least] * (count - 1), total - largest - least * (count - 1)
    while rest > 0:
        candidates = [i for i in range(1, count) if given[i] < largest] or [i for i in range(1, count) if given[i] < reach]
        mass, remaining = sum([loads[i] for i in candidates]), rest
        for i in candidates:
            extra = min(reach - given[i], max(1, remaining * loads[i] // mass), rest)
            given[i] = given[i] + extra
            rest = rest - extra
    return np.array(given)


def bell_draw(key, dims, width, reach, pieces=(), kind=jnp.bfloat16):
    result = jax.random.normal(key, dims, jnp.float32) * width
    if len(pieces) > 0:
        result = level_of(key, dims, pieces, -0.22, 0.18) * result
    return jnp.clip(result, min=-reach, max=reach).astype(kind)


def setup_inputs(seed: int = 0) -> dict:
    keys = jax.random.split(jax.random.key(seed), 17)
    residual_in = bell_draw(keys[0], (TOKENS, D), 1.0, 6.0, ((0, 128),))
    rec_state = bell_draw(keys[1], (TOKENS, HEADS, HEAD, HEAD), 1.0, 6.0, ((0, 128), (1, 4)))
    mix_gain = jnp.clip(1.0 + 0.18 * jax.random.normal(keys[2], (D,), jnp.float32), 0.1, 1.9)
    w_query = bell_draw(keys[3], (D, D), D ** -0.5, 0.15625, ((0, 4), (1, 128)))
    w_forget = bell_draw(keys[4], (D, D), D ** -0.5, 0.15625, ((0, 4), (1, 128)))
    w_input = bell_draw(keys[5], (D, D), D ** -0.5, 0.15625, ((0, 4), (1, 128)))
    w_gate = bell_draw(keys[6], (D, D), D ** -0.5, 0.15625, ((0, 4), (1, 128)))
    lower_bound = jnp.clip(0.9 * jax.random.uniform(keys[7], (D,), jnp.float32) ** level_of(keys[7], (D,), ((0, 4),), -0.2, 0.2), 0.0, 0.9)
    head_gain = jnp.clip(1.0 + 0.18 * jax.random.normal(keys[8], (HEAD,), jnp.float32), 0.1, 1.9)
    w_out = bell_draw(keys[9], (D, D), D ** -0.5, 0.15625, ((0, 4), (1, 128)))
    ffn_gain = jnp.clip(1.0 + 0.18 * jax.random.normal(keys[10], (D,), jnp.float32), 0.1, 1.9)
    route_ids_keys = jax.random.split(jax.random.fold_in(keys[11], 1), TOKENS // SEQ_DEV)
    route_ids_turns = jax.random.permutation(jax.random.fold_in(keys[11], 3), TOKENS // SEQ_DEV)
    route_ids = jax.vmap(lambda own, number: shared_out(jax.random.fold_in(keys[11], 2), own, number, SEQ_DEV, EXPERTS, TOPK, CAP, 2))(route_ids_keys, route_ids_turns).reshape((TOKENS, TOPK))
    route_weight = jnp.clip(jnp.exp(math.log(1.0) - 1.609438 * jax.random.uniform(keys[12], (TOKENS, TOPK), jnp.float32) ** level_of(keys[12], (TOKENS, TOPK), ((0, 128),), -0.2, 0.2)), 0.2, 1.0)
    expert_gate = bell_draw(keys[13], (EXPERTS, D, FF), D ** -0.5, 0.15625, ((0, 128), (2, 4)))
    expert_up = bell_draw(keys[14], (EXPERTS, D, FF), D ** -0.5, 0.15625, ((0, 128), (2, 4)))
    expert_down = bell_draw(keys[15], (EXPERTS, FF, D), FF ** -0.5, 0.25, ((0, 128), (1, 4)))
    return dict(residual_in=residual_in, rec_state=rec_state, mix_gain=mix_gain, w_query=w_query, w_forget=w_forget, w_input=w_input, w_gate=w_gate, lower_bound=lower_bound, head_gain=head_gain, w_out=w_out, ffn_gain=ffn_gain, route_ids=route_ids, route_weight=route_weight, expert_gate=expert_gate, expert_up=expert_up, expert_down=expert_down)


rms_eps = 1e-06

def rms_scale(values, gain):
    return values * lax.rsqrt(lax.optimization_barrier(jnp.mean(values * values, axis=-1, keepdims=True)) + rms_eps) * gain

def rounded(values):
    return lax.optimization_barrier(values.astype(jnp.bfloat16)).astype(jnp.float32)

def recurrence(lower_bound, head_gain, state_block, query_raw, forget_raw, input_raw, gate_raw):
    seq_count = state_block.shape[0]
    heads_local = state_block.shape[1]
    head_size = state_block.shape[2]
    head_shape = (seq_count, heads_local, head_size)
    forget = lower_bound + (1.0 - lower_bound) * jax.nn.sigmoid(forget_raw)
    query_act = jax.nn.silu(query_raw).reshape(head_shape)
    key_act = (1.0 - forget).reshape(head_shape)
    forget_heads = forget.reshape(head_shape)
    value_act = input_raw.reshape(head_shape)
    state_next = forget_heads[:, :, :, None] * state_block.astype(jnp.float32) + key_act[:, :, :, None] * value_act[:, :, None, :]
    readout = jnp.einsum('shk,shkv->shv', query_act, state_next, precision=lax.Precision.HIGHEST)
    gate_heads = jax.nn.silu(gate_raw).reshape(head_shape)
    heads_out = rms_scale(readout, head_gain) * gate_heads
    return (state_next.astype(jnp.bfloat16), heads_out.reshape(seq_count, heads_local * head_size).astype(jnp.bfloat16))

def reference(residual_in, rec_state, mix_gain, w_query, w_forget, w_input, w_gate, lower_bound, head_gain, w_out, ffn_gain, route_ids, route_weight, expert_gate, expert_up, expert_down):
    residual = residual_in.astype(jnp.float32)
    normed = rms_scale(residual, mix_gain).astype(jnp.bfloat16)
    projected = [rounded(jnp.dot(normed, weight, preferred_element_type=jnp.float32)) for weight in (w_query, w_forget, w_input, w_gate)]

    def to_blocks(values):
        return values.reshape((N_EP, SEQ_DEV) + values.shape[1:])

    def per_block(blocks):
        return recurrence(lower_bound, head_gain, blocks[0], blocks[1], blocks[2], blocks[3], blocks[4])
    state_next, heads_out = lax.map(per_block, (to_blocks(rec_state), to_blocks(projected[0]), to_blocks(projected[1]), to_blocks(projected[2]), to_blocks(projected[3])))
    new_state = state_next.reshape(rec_state.shape)
    heads_out = heads_out.reshape(TOKENS, D)
    mixed = jnp.dot(heads_out, w_out, preferred_element_type=jnp.float32)
    after_mix = rounded(residual + mixed)
    normed_ffn = rms_scale(after_mix, ffn_gain).astype(jnp.bfloat16)

    def one_slot(slot_args):
        row_values = slot_args[0]
        expert_id = slot_args[1]
        gate_part = jnp.dot(row_values, expert_gate[expert_id], preferred_element_type=jnp.float32)
        up_part = jnp.dot(row_values, expert_up[expert_id], preferred_element_type=jnp.float32)
        hidden = (jax.nn.silu(gate_part) * up_part).astype(jnp.bfloat16)
        return jnp.dot(hidden, expert_down[expert_id], preferred_element_type=jnp.float32).astype(jnp.bfloat16)
    slot_rows = jnp.repeat(normed_ffn, TOPK, axis=0)
    expert_rows = lax.map(one_slot, (slot_rows, route_ids.reshape(-1).astype(jnp.int32)))
    expert_sum = lax.optimization_barrier(jnp.sum(route_weight[:, :, None] * expert_rows.reshape(TOKENS, TOPK, D).astype(jnp.float32), axis=1))
    layer_out = (after_mix + expert_sum).astype(jnp.bfloat16)
    return (layer_out, new_state)
```

```python
import jax
import jax.numpy as jnp
from jax import lax
from jax.experimental import pallas as pl
from jax.experimental.pallas import tpu as pltpu
from jax.sharding import Mesh
from jax.sharding import PartitionSpec as P

EP = ("ep_0", "ep_1", "ep_2")
EPS = 1e-06
BF = jnp.bfloat16
F32 = jnp.float32
NZ, NX, NC, NY = 16, 4, 2, 4
XC = NX * NC
D, Q, SEQ, HEAD, HL, FQ, TOPK = 1536, 384, 15, 128, 3, 128, 6
COLS = 12


def dot(a, b):
    return lax.dot_general(a, b, (((1,), (0,)), ((), ())), preferred_element_type=F32)


def dot_t(a, b):
    return lax.dot_general(a, b, (((1,), (1,)), ((), ())), preferred_element_type=F32)


def iota(shape, dim):
    return lax.broadcasted_iota(jnp.int32, shape, dim)


def split_two(x):
    hi = x.astype(BF)
    return hi, (x - hi.astype(F32)).astype(BF)


def sigmoid(x):
    return 1.0 / (1.0 + jnp.exp(-x))


def kernel(
    res_ref,
    mix_gain_ref,
    w_ref,
    lower_ref,
    head_gain_ref,
    ffn_gain_ref,
    ids_ref,
    rw_ref,
    state_hbm,
    eg_hbm,
    eu_hbm,
    ed_hbm,
    out_ref,
    new_state_hbm,
    wz,
    wo,
    tok,
    psend,
    precv,
    perm_in,
    state_v,
    state_o,
    cols,
    rows_s,
    read_s,
    ho,
    rsend,
    rrecv,
    ssend,
    srecv,
    res_s,
    ids_s,
    rw_s,
    tz,
    xsend,
    xf,
    hf,
    dq,
    wg_v,
    wu_v,
    osend,
    orecv,
    zsend,
    zrecv,
    z1s,
    z1r,
    toks,
    tokr,
    ps,
    pr,
    wos,
    wor,
    rss,
    rsr,
    sss,
    ssr,
    z2s,
    z2r,
    xs,
    xr,
    ys,
    yr,
    hs,
    hr,
    ds_,
    dr,
    os_,
    or_,
    rets,
    retr,
    local,
):
    z = lax.axis_index("ep_0")
    x = lax.axis_index("ep_1")
    c = lax.axis_index("ep_2")
    y = lax.axis_index("tp")
    me = x * NC + c
    pending = []

    def dev(dz=0, dx=0, dc=0, dy=0):
        return {
            "ep_0": lax.rem(z + dz + NZ, NZ),
            "ep_1": lax.rem(x + dx + NX, NX),
            "ep_2": lax.rem(c + dc + NC, NC),
            "tp": lax.rem(y + dy + NY, NY),
        }

    def send(src, dst, ss, rs, to):
        copy = pltpu.make_async_remote_copy(
            src_ref=src,
            dst_ref=dst,
            send_sem=ss,
            recv_sem=rs,
            device_id=to,
            device_id_type=pl.DeviceIdType.MESH,
        )
        copy.start()
        pending.append(copy)

    def arrive(dst, ss, rs):
        pltpu.make_async_remote_copy(
            src_ref=dst,
            dst_ref=dst,
            send_sem=ss,
            recv_sem=rs,
            device_id=dev(),
            device_id_type=pl.DeviceIdType.MESH,
        ).wait_recv()

    def zi(d):
        return lax.rem(z + d + NZ, NZ)

    def yi(d):
        return lax.rem(y + d + NY, NY)

    groups = [(dx, dc) for dx in range(NX) for dc in range(NC)]

    def xc_to(g):
        return lax.rem(x + g[0], NX) * NC + lax.rem(c + g[1], NC)

    def xc_from(g):
        return lax.rem(x - g[0] + NX, NX) * NC + lax.rem(c - g[1] + NC, NC)

    loads = [
        pltpu.make_async_copy(state_hbm, state_v, local.at[0]),
        pltpu.make_async_copy(eg_hbm, wg_v, local.at[1]),
        pltpu.make_async_copy(eu_hbm, wu_v, local.at[2]),
    ]

    def quarter(ref, part):
        return ref.at[:, pl.ds(pl.multiple_of(part * Q, Q), Q)]

    own_down = pltpu.make_async_copy(quarter(ed_hbm, y), dq.at[y], local.at[3])

    barrier = pltpu.get_barrier_semaphore()
    peers = [dict(dz=d) for d in range(1, NZ)]
    for g in groups:
        for dy in range(NY):
            if g != (0, 0) or dy:
                peers.append(dict(dx=g[0], dc=g[1], dy=dy))
    for p in peers:
        pl.semaphore_signal(
            barrier, inc=1, device_id=dev(**p), device_id_type=pl.DeviceIdType.MESH
        )

    res_s[...] = jnp.zeros_like(res_s)
    res_s[0:SEQ, :] = res_ref[...].astype(F32)
    own_w = pltpu.make_async_copy(w_ref, wz.at[z], local.at[4])
    own_w.start()
    res = res_s[...]
    scale = lax.rsqrt(jnp.mean(res * res, axis=-1, keepdims=True) + EPS)
    own = pl.ds(pl.multiple_of(y * Q, Q), Q)
    tok[me] = (res_s[:, own] * scale * mix_gain_ref[:, own]).astype(BF)
    own_w.wait()
    pl.semaphore_wait(barrier, len(peers))

    def z_start(buf, ss, rs):
        for k, d in ((2, 4), (3, -4), (0, 1), (1, -1), (4, 2), (5, -2)):
            send(buf.at[z], buf.at[z], ss.at[k], rs.at[k], dev(dz=d))

    def z_finish(buf, ss, rs, first, second):
        def block(d, part=None):
            ref = buf.at[zi(d)]
            return ref if part is None else ref.at[part]

        def pass_on(k, d, to, part=None):
            send(block(d, part), block(d, part), ss.at[k], rs.at[k], dev(dz=to))

        def got(k, d, part=None):
            arrive(block(d, part), ss.at[k], rs.at[k])

        got(2, -4)
        pass_on(6, -4, 4, first)
        got(3, 4)
        pass_on(10, 4, -4, second)
        for k, d, to in ((7, -4, 1), (8, -4, -1), (9, -4, 2), (11, 4, 1), (12, 4, -1), (13, 4, -2)):
            pass_on(k, d, to)
        got(6, 8, first)
        got(10, 8, second)
        pass_on(14, 8, 1)
        pass_on(15, 8, -1)
        for k, d in (
            (0, -1), (1, 1), (4, -2), (5, 2), (7, -5), (8, -3),
            (9, -6), (11, 3), (12, 5), (13, 6), (14, 7), (15, 9),
        ):
            got(k, d)

    z_start(wz, z1s, z1r)
    for i, g in enumerate(groups[1:], 1):
        send(tok.at[me], tok.at[me], toks.at[i], tokr.at[i], dev(dx=g[0], dc=g[1]))
    for copy in loads:
        copy.start()
    own_down.start()
    for k in range(1, NY):
        send(quarter(ed_hbm, yi(k)), dq.at[y], ds_.at[k], dr.at[k], dev(dy=k))

    ids_s[...] = jnp.full_like(ids_s, -1)
    ids_s[0:SEQ, 0:TOPK] = ids_ref[...]
    rw_s[...] = jnp.zeros_like(rw_s)
    rw_s[0:SEQ, 0:TOPK] = rw_ref[...]
    ids, rw = ids_s[...], rw_s[...]
    lane = iota((16, 256), 1)
    expert, slot = lane // 2, lane % 2
    row = iota((16, 256), 0).astype(F32)
    named = jnp.zeros((16, 256), F32)
    weight = jnp.zeros((16, 256), F32)
    for j in range(TOPK):
        hit = ids[:, j : j + 1] == expert
        named = jnp.where(hit, 1.0, named)
        weight = jnp.where(hit, rw[:, j : j + 1], weight)
    low = jnp.min(jnp.where(named > 0.5, row, 99.0), axis=0, keepdims=True)
    high = jnp.max(jnp.where(named > 0.5, row, -1.0), axis=0, keepdims=True)
    second = jnp.where(high > low, high, 99.0)
    table = jnp.where(slot[0:1] == 0, low, second)
    combine = jnp.where(row == table, weight, 0.0)
    comb_hi, comb_lo = split_two(combine)

    k_id = iota((1024, 1), 0)
    k_xc, k_in = k_id // 128, k_id % 128
    k_q, k_pj = k_in // 64, k_in % 64
    k_p, k_j = k_pj // COLS, k_pj % COLS
    target = jnp.where(k_pj < 48, k_p * 256 + k_q * 96 + COLS * k_xc + k_j, -1)
    order_in = jnp.where(iota((1024, 1024), 1) == target, 1.0, 0.0).astype(BF)
    perm_in[...] = order_in

    z_finish(wz, z1s, z1r, (pl.ds(0, 32),), (pl.ds(32, 32),))

    wo_own = wz.at[:, pl.ds(48, 16), :]
    own_wo = pltpu.make_async_copy(wo_own, wo.at[me], local.at[5])
    own_wo.start()
    for i, g in enumerate(groups[1:], 1):
        arrive(tok.at[xc_from(g)], toks.at[i], tokr.at[i])
    tokens = tok[...].reshape(XC * 16, Q)

    pairs = [(g, dy) for dy in range(NY) for g in groups]
    for k in range(NY):
        part = yi(k)
        block = wz[pl.ds(4 * part, 4)].reshape(256, Q)
        psend[part] = dot_t(tokens, block).astype(BF).reshape(XC, 16, 256)
    precv[y, me] = psend[y, me]
    for i, (g, dy) in enumerate(pairs):
        if i == 0:
            continue
        send(
            psend.at[yi(dy), xc_to(g)],
            precv.at[y, me],
            ps.at[i],
            pr.at[i],
            dev(dx=g[0], dc=g[1], dy=dy),
        )
    for dx in range(1, NX):
        send(wo_own, wo.at[me], wos.at[dx], wor.at[dx], dev(dx=dx))
    send(wo_own, wo.at[me], wos.at[0], wor.at[0], dev(dc=1))

    for i, (g, dy) in enumerate(pairs):
        if i:
            arrive(precv.at[yi(-dy), xc_from(g)], ps.at[i], pr.at[i])
    halves = [[], []]
    for e in range(XC):
        total = precv[0, e].astype(F32)
        for k in range(1, NY):
            total = total + precv[k, e].astype(F32)
        total = total.astype(BF)
        halves[0].append(total[:, 0:128])
        halves[1].append(total[:, 128:256])
    stacked = jnp.concatenate(
        [jnp.concatenate(half, axis=1) for half in halves], axis=0
    )
    ordered = dot(stacked, perm_in[...])
    narrow = iota((16, 128), 1) < 64
    proj = []
    for p in range(4):
        a = ordered[0:16, 256 * p : 256 * p + 256]
        b = ordered[16:32, 256 * p : 256 * p + 256]
        b0 = pltpu.roll(b[:, 0:128], 64, 1)
        b1 = pltpu.roll(b[:, 128:256], 64, 1)
        proj.append(
            [a[:, 0:128], jnp.where(narrow, a[:, 128:256], b0), jnp.where(narrow, b0, b1)]
        )
    gates = []
    for h in range(HL):
        lower = lower_ref[:, h * HEAD : (h + 1) * HEAD]
        query = proj[0][h] * sigmoid(proj[0][h])
        forget = lower + (1.0 - lower) * sigmoid(proj[1][h])
        for n, values in enumerate((query, forget)):
            tall = jnp.concatenate([values, jnp.zeros((112, 128), F32)], axis=0)
            cols[n, h] = jnp.transpose(tall)
        rows_s[h] = proj[2][h]
        gates.append(proj[3][h] * sigmoid(proj[3][h]))

    loads[0].wait()
    read_s[...] = jnp.zeros_like(read_s)

    def one_head(h, _):
        queries, forgets, values = cols[0, h], cols[1, h], rows_s[h]
        for s in range(SEQ):
            f = forgets[:, s : s + 1]
            q = queries[:, s : s + 1]
            v = values[s : s + 1, :]
            nxt = f * state_v[s, h].astype(F32) + (1.0 - f) * v
            state_o[s, h] = nxt.astype(BF)
            read_s[h, s : s + 1, :] = jnp.sum(q * nxt, axis=0, keepdims=True)
        return 0

    lax.fori_loop(0, HL, one_head, 0)
    store = pltpu.make_async_copy(state_o, new_state_hbm, local.at[6])
    store.start()
    for h in range(HL):
        r = read_s[h]
        r = r * lax.rsqrt(jnp.mean(r * r, axis=-1, keepdims=True) + EPS)
        ho[:, h * HEAD : (h + 1) * HEAD] = (r * head_gain_ref[...] * gates[h]).astype(BF)

    for dx in range(1, NX):
        src = lax.rem(x - dx + NX, NX) * NC + c
        arrive(wo.at[src], wos.at[dx], wor.at[dx])
        send(wo.at[src], wo.at[src], wos.at[NX + dx], wor.at[NX + dx], dev(dc=1))
    other = 1 - c
    arrive(wo.at[x * NC + other], wos.at[0], wor.at[0])
    for dx in range(1, NX):
        src = lax.rem(x - dx + NX, NX) * NC + other
        arrive(wo.at[src], wos.at[NX + dx], wor.at[NX + dx])
    own_wo.wait()
    heads = ho[...]
    for k in (1, 2, 3, 0):
        part = yi(k)
        block = wo[:, pl.ds(4 * part, 4)].reshape(512, Q)
        rsend[part] = dot_t(heads, block).astype(BF)
        if k:
            send(rsend.at[part], rrecv.at[y], rss.at[k], rsr.at[k], dev(dy=k))
    rrecv[y] = rsend[y]
    o_id = iota((512, 1), 0)
    o_xc, o_q, o_j = o_id // 64, (o_id // 16) % 4, o_id % 16
    o_to = jnp.where(o_j < COLS, 96 * o_q + COLS * o_xc + o_j, -1)
    order_out = jnp.where(iota((512, Q), 1) == o_to, 1.0, 0.0).astype(BF)
    for k in range(1, NY):
        arrive(rrecv.at[yi(-k)], rss.at[k], rsr.at[k])
    total = rrecv[0].astype(F32)
    for k in range(1, NY):
        total = total + rrecv[k].astype(F32)
    both = dot(jnp.concatenate(split_two(total), axis=0), order_out)
    after = (res_s[:, own] + (both[0:16] + both[16:32])).astype(BF).astype(F32)
    square = jnp.sum(after * after, axis=-1, keepdims=True)
    ssend[...] = jnp.broadcast_to(square, (16, 128))
    srecv[y] = ssend[...]
    for k in range(1, NY):
        send(ssend, srecv.at[y], sss.at[k], ssr.at[k], dev(dy=k))
    gained = after * ffn_gain_ref[:, own]
    table_row = jnp.concatenate([table, jnp.zeros((1, 128), F32)], axis=1)
    is_table = iota((16, Q), 0) == SEQ
    for k in range(1, NY):
        arrive(srecv.at[yi(-k)], sss.at[k], ssr.at[k])
    square = srecv[0] + srecv[1] + srecv[2] + srecv[3]
    inverse = lax.rsqrt(square[:, 0:1] * (1.0 / D) + EPS)
    tz[z] = jnp.where(is_table, table_row, gained * inverse).astype(BF)

    z_start(tz, z2s, z2r)
    r_id, l_id = iota((256, 256), 0), iota((256, 256), 1)
    spread = jnp.where((r_id // 16 == l_id // 16) & (l_id % 16 == SEQ), 1.0, 0.0).astype(BF)
    mine = jnp.where(iota((16, 256), 1) == 16 * z + iota((16, 256), 0), 1.0, 0.0).astype(BF)
    same = iota((16, 256), 0) == iota((16, 256), 1) // 16
    token = (iota((16, 256), 1) % 16).astype(F32)
    loads[1].wait()
    loads[2].wait()
    z_finish(tz, z2s, z2r, (slice(None), pl.ds(0, 256)), (slice(None), pl.ds(256, 128)))
    flat = tz[...].reshape(256, Q)
    tables = dot(spread, flat[:, 0:256]).astype(BF)
    wanted = dot_t(mine, tables)
    hit = jnp.where(wanted == token, 1.0, 0.0)
    same_f = jnp.where(same, 1.0, 0.0)
    pick = (hit[:, None, :] * same_f[None, :, :]).reshape(256, 256).astype(BF)
    xsend[...] = dot(pick, flat).astype(BF).reshape(XC, 32, Q)
    xf[y, me] = xsend[me]
    for i, g in enumerate(groups[1:], 1):
        send(xsend.at[xc_to(g)], xf.at[y, me], xs.at[i], xr.at[i], dev(dx=g[0], dc=g[1]))
    for i, g in enumerate(groups):
        chunk = xf.at[y, xc_from(g)]
        if i:
            arrive(chunk, xs.at[i], xr.at[i])
        send(chunk, chunk, ys.at[0, i], yr.at[0, i], dev(dy=1))
        send(chunk, chunk, ys.at[1, i], yr.at[1, i], dev(dy=-1))

    def weights_of(part):
        at = pl.ds(pl.multiple_of(part * Q, Q), Q)
        return wg_v[at, :], wu_v[at, :]

    def add_part(part, sums):
        rows = xf[part].reshape(256, Q)
        a, b = weights_of(part)
        return sums[0] + dot(rows, a), sums[1] + dot(rows, b)

    sums = add_part(y, (jnp.zeros((256, FQ), F32), jnp.zeros((256, FQ), F32)))
    for i, g in enumerate(groups):
        left = xf.at[yi(-1), xc_from(g)]
        right = xf.at[yi(1), xc_from(g)]
        arrive(left, ys.at[0, i], yr.at[0, i])
        if i < 4:
            send(left, left, ys.at[2, i], yr.at[2, i], dev(dy=1))
        arrive(right, ys.at[1, i], yr.at[1, i])
        if i >= 4:
            send(right, right, ys.at[2, i], yr.at[2, i], dev(dy=-1))
    sums = add_part(yi(-1), sums)
    sums = add_part(yi(1), sums)
    for i, g in enumerate(groups):
        arrive(xf.at[yi(2), xc_from(g)], ys.at[2, i], yr.at[2, i])
    gate, up = add_part(yi(2), sums)
    hf[y] = (gate * sigmoid(gate) * up).astype(BF)

    send(hf.at[y], hf.at[y], hs.at[0], hr.at[0], dev(dy=1))
    send(hf.at[y], hf.at[y], hs.at[1], hr.at[1], dev(dy=-1))
    own_down.wait()
    for k in range(1, NY):
        arrive(dq.at[yi(-k)], ds_.at[k], dr.at[k])
    down = dot(hf[y], dq[y])
    top, bottom = pl.ds(0, 128), pl.ds(128, 128)
    left = hf.at[yi(-1)]
    right = hf.at[yi(1)]
    arrive(left, hs.at[0], hr.at[0])
    send(left.at[top], left.at[top], hs.at[2], hr.at[2], dev(dy=1))
    arrive(right, hs.at[1], hr.at[1])
    send(right.at[bottom], right.at[bottom], hs.at[3], hr.at[3], dev(dy=-1))
    down = down + dot(hf[yi(-1)], dq[yi(-1)]) + dot(hf[yi(1)], dq[yi(1)])
    far = hf.at[yi(2)]
    arrive(far.at[top], hs.at[2], hr.at[2])
    arrive(far.at[bottom], hs.at[3], hr.at[3])
    down = down + dot(hf[yi(2)], dq[yi(2)])
    osend[...] = down.astype(BF).reshape(XC, 32, Q)

    orecv[me] = osend[me]
    for i, g in enumerate(groups[1:], 1):
        send(osend.at[xc_to(g)], orecv.at[me], os_.at[i], or_.at[i], dev(dx=g[0], dc=g[1]))
    to_z, to_e = r_id // 16, r_id % 16
    source = (to_e // 2) * 32 + (to_e % 2) * 16 + to_z
    turn = jnp.where(l_id == source, 1.0, 0.0).astype(BF)
    for i, g in enumerate(groups[1:], 1):
        arrive(orecv.at[xc_from(g)], os_.at[i], or_.at[i])
    zsend[...] = dot(turn, orecv[...].reshape(256, Q)).astype(BF).reshape(NZ, 16, Q)
    zrecv[z] = zsend[z]
    for d in (8, 7, 9, 6, 10, 5, 11, 4, 12, 3, 13, 2, 14, 1, 15):
        send(zsend.at[zi(d)], zrecv.at[z], rets.at[d], retr.at[d], dev(dz=d))
    for d in range(1, NZ):
        arrive(zrecv.at[zi(-d)], rets.at[d], retr.at[d])
    back = zrecv[...].reshape(256, Q)
    both = dot(jnp.concatenate([comb_hi, comb_lo], axis=0), back)
    result = (after + (both[0:16] + both[16:32])).astype(BF)
    out_ref[...] = result[0:SEQ, :]
    store.wait()
    for copy in pending:
        copy.wait_send()


def shards(
    residual_in,
    rec_state,
    mix_gain,
    w_query,
    w_forget,
    w_input,
    w_gate,
    lower_bound,
    head_gain,
    w_out,
    ffn_gain,
    route_ids,
    route_weight,
    expert_gate,
    expert_up,
    expert_down,
):
    columns = jnp.concatenate(
        [w_query, w_forget, w_input, w_gate, w_out, jnp.zeros((Q, 4), BF)], axis=1
    ).T
    vmem = pl.BlockSpec(memory_space=pltpu.VMEM)
    hbm = pl.BlockSpec(memory_space=pl.ANY)
    dma = pltpu.SemaphoreType.DMA
    out = pl.pallas_call(
        kernel,
        out_shape=(
            jax.ShapeDtypeStruct((SEQ, Q), BF),
            jax.ShapeDtypeStruct(rec_state.shape, BF),
        ),
        in_specs=[vmem] * 8 + [hbm] * 4,
        out_specs=(vmem, hbm),
        scratch_shapes=[
            pltpu.VMEM((NZ, 64, Q), BF),
            pltpu.VMEM((XC, NZ, 16, Q), BF),
            pltpu.VMEM((XC, 16, Q), BF),
            pltpu.VMEM((NY, XC, 16, 256), BF),
            pltpu.VMEM((NY, XC, 16, 256), BF),
            pltpu.VMEM((1024, 1024), BF),
            pltpu.VMEM((SEQ, HL, HEAD, HEAD), BF),
            pltpu.VMEM((SEQ, HL, HEAD, HEAD), BF),
            pltpu.VMEM((2, HL, HEAD, 128), F32),
            pltpu.VMEM((HL, 16, HEAD), F32),
            pltpu.VMEM((HL, 16, HEAD), F32),
            pltpu.VMEM((16, Q), BF),
            pltpu.VMEM((NY, 16, 512), BF),
            pltpu.VMEM((NY, 16, 512), BF),
            pltpu.VMEM((16, 128), F32),
            pltpu.VMEM((NY, 16, 128), F32),
            pltpu.VMEM((16, D), F32),
            pltpu.VMEM((16, 128), jnp.int32),
            pltpu.VMEM((16, 128), F32),
            pltpu.VMEM((NZ, 16, Q), BF),
            pltpu.VMEM((XC, 32, Q), BF),
            pltpu.VMEM((NY, XC, 32, Q), BF),
            pltpu.VMEM((NY, 256, FQ), BF),
            pltpu.VMEM((NY, FQ, Q), BF),
            pltpu.VMEM((D, FQ), BF),
            pltpu.VMEM((D, FQ), BF),
            pltpu.VMEM((XC, 32, Q), BF),
            pltpu.VMEM((XC, 32, Q), BF),
            pltpu.VMEM((NZ, 16, Q), BF),
            pltpu.VMEM((NZ, 16, Q), BF),
        ]
        + [
            dma((n,))
            for n in (16, 16, 8, 8, 32, 32, 8, 8, 4, 4, 4, 4, 16, 16, 8, 8)
        ]
        + [dma((3, 8)), dma((3, 8))]
        + [dma((n,)) for n in (4, 4, 4, 4, 8, 8, 16, 16, 8)],
        compiler_params=pltpu.CompilerParams(
            collective_id=0, has_side_effects=True, vmem_limit_bytes=48 * 1024 * 1024
        ),
    )(
        residual_in,
        mix_gain.reshape(1, D),
        columns,
        lower_bound.reshape(1, Q),
        head_gain.reshape(1, HEAD),
        ffn_gain.reshape(1, D),
        route_ids,
        route_weight,
        rec_state,
        expert_gate.reshape(D, FQ),
        expert_up.reshape(D, FQ),
        expert_down.reshape(FQ, D),
    )
    return out


def solution(mesh):
    split = Mesh(mesh.devices.reshape(NZ, NX, NC, NY), ("ep_0", "ep_1", "ep_2", "tp"))
    in_specs = (
        P(EP, None),
        P(EP, "tp", None, None),
        P(),
        P("tp", EP),
        P("tp", EP),
        P("tp", EP),
        P("tp", EP),
        P("tp"),
        P(),
        P("tp", EP),
        P(),
        P(EP, None),
        P(EP, None),
        P(EP, None, "tp"),
        P(EP, None, "tp"),
        P(EP, "tp", None),
    )
    out_specs = (P(EP, "tp"), P(EP, "tp", None, None))
    return jax.shard_map(
        shards, mesh=split, in_specs=in_specs, out_specs=out_specs, check_vma=False
    )
```

```python
import jax
import jax.numpy as jnp
from jax import lax
from jax.experimental import pallas as pl
from jax.experimental.pallas import tpu as pltpu
from jax.sharding import Mesh
from jax.sharding import PartitionSpec as P

EP = ("ep_0", "ep_1", "ep_2")
EPS = 1e-06
BF = jnp.bfloat16
F32 = jnp.float32
NZ, NX, NC, NY = 16, 4, 2, 4
XC = NX * NC
D, Q, SEQ, HEAD, HL, FQ, TOPK = 1536, 384, 15, 128, 3, 128, 6
COLS = 12


def dot(a, b):
    return lax.dot_general(a, b, (((1,), (0,)), ((), ())), preferred_element_type=F32)


def dot_t(a, b):
    return lax.dot_general(a, b, (((1,), (1,)), ((), ())), preferred_element_type=F32)


def iota(shape, dim):
    return lax.broadcasted_iota(jnp.int32, shape, dim)


def split_two(x):
    hi = x.astype(BF)
    return hi, (x - hi.astype(F32)).astype(BF)


def sigmoid(x):
    return 1.0 / (1.0 + jnp.exp(-x))


def kernel(
    res_hbm,
    wq_hbm,
    wf_hbm,
    wi_hbm,
    wg_hbm,
    wo_hbm,
    mix_gain_hbm,
    lower_hbm,
    head_gain_hbm,
    ffn_gain_hbm,
    ids_hbm,
    rw_hbm,
    state_hbm,
    eg_hbm,
    eu_hbm,
    ed_hbm,
    out_ref,
    new_state_hbm,
    res_ref,
    w_v,
    w_all,
    mix_gain_v,
    lower_v,
    head_gain_v,
    ffn_gain_v,
    ids_v,
    rw_v,
    wz,
    wo,
    tok,
    psend,
    precv,
    perm_in,
    state_v,
    state_o,
    cols,
    rows_s,
    read_s,
    ho,
    rsend,
    rrecv,
    ssend,
    srecv,
    res_s,
    ids_s,
    rw_s,
    tz,
    xsend,
    xf,
    hf,
    dq,
    wg_v,
    wu_v,
    osend,
    orecv,
    zsend,
    zrecv,
    z1s,
    z1r,
    toks,
    tokr,
    ps,
    pr,
    wos,
    wor,
    rss,
    rsr,
    sss,
    ssr,
    z2s,
    z2r,
    xs,
    xr,
    ys,
    yr,
    hs,
    hr,
    ds_,
    dr,
    os_,
    or_,
    rets,
    retr,
    local,
):
    z = lax.axis_index("ep_0")
    x = lax.axis_index("ep_1")
    c = lax.axis_index("ep_2")
    y = lax.axis_index("tp")
    me = x * NC + c
    pending = []

    def dev(dz=0, dx=0, dc=0, dy=0):
        return {
            "ep_0": lax.rem(z + dz + NZ, NZ),
            "ep_1": lax.rem(x + dx + NX, NX),
            "ep_2": lax.rem(c + dc + NC, NC),
            "tp": lax.rem(y + dy + NY, NY),
        }

    def send(src, dst, ss, rs, to):
        copy = pltpu.make_async_remote_copy(
            src_ref=src,
            dst_ref=dst,
            send_sem=ss,
            recv_sem=rs,
            device_id=to,
            device_id_type=pl.DeviceIdType.MESH,
        )
        copy.start()
        pending.append(copy)

    def arrive(dst, ss, rs):
        pltpu.make_async_remote_copy(
            src_ref=dst,
            dst_ref=dst,
            send_sem=ss,
            recv_sem=rs,
            device_id=dev(),
            device_id_type=pl.DeviceIdType.MESH,
        ).wait_recv()

    def zi(d):
        return lax.rem(z + d + NZ, NZ)

    def yi(d):
        return lax.rem(y + d + NY, NY)

    groups = [(dx, dc) for dx in range(NX) for dc in range(NC)]

    def xc_to(g):
        return lax.rem(x + g[0], NX) * NC + lax.rem(c + g[1], NC)

    def xc_from(g):
        return lax.rem(x - g[0] + NX, NX) * NC + lax.rem(c - g[1] + NC, NC)

    loads = [
        pltpu.make_async_copy(state_hbm, state_v, local.at[0]),
        pltpu.make_async_copy(eg_hbm, wg_v, local.at[1]),
        pltpu.make_async_copy(eu_hbm, wu_v, local.at[2]),
    ]
    early = [
        (wq_hbm, w_v.at[0]),
        (wf_hbm, w_v.at[1]),
        (wi_hbm, w_v.at[2]),
        (wg_hbm, w_v.at[3]),
        (wo_hbm, w_v.at[4]),
        (res_hbm, res_ref),
        (mix_gain_hbm, mix_gain_v),
        (lower_hbm, lower_v),
        (head_gain_hbm, head_gain_v),
        (ffn_gain_hbm, ffn_gain_v),
        (ids_hbm, ids_v),
        (rw_hbm, rw_v),
    ]
    early = [
        pltpu.make_async_copy(src, dst, local.at[8 + n])
        for n, (src, dst) in enumerate(early)
    ]
    for copy in early:
        copy.start()

    def quarter(ref, part):
        return ref.at[:, pl.ds(pl.multiple_of(part * Q, Q), Q)]

    own_down = pltpu.make_async_copy(quarter(ed_hbm, y), dq.at[y], local.at[3])

    barrier = pltpu.get_barrier_semaphore()
    peers = [dict(dz=d) for d in range(1, NZ)]
    for g in groups:
        for dy in range(NY):
            if g != (0, 0) or dy:
                peers.append(dict(dx=g[0], dc=g[1], dy=dy))
    for p in peers:
        pl.semaphore_signal(
            barrier, inc=1, device_id=dev(**p), device_id_type=pl.DeviceIdType.MESH
        )

    res_s[...] = jnp.zeros_like(res_s)
    w_all[...] = jnp.zeros_like(w_all)
    for copy in early:
        copy.wait()
    for n in range(5):
        w_all[n * COLS : (n + 1) * COLS, :] = w_v[n].astype(F32)
    wz[z] = w_all[...].astype(BF)
    res_s[0:SEQ, :] = res_ref[...].astype(F32)
    res = res_s[...]
    mix_gain = mix_gain_v[pl.ds(pl.multiple_of(y * Q, Q), Q)].reshape(1, Q)
    ffn_gain = ffn_gain_v[pl.ds(pl.multiple_of(y * Q, Q), Q)].reshape(1, Q)
    lower_all = lower_v[...].reshape(1, Q)
    head_gain = head_gain_v[...].reshape(1, HEAD)
    scale = lax.rsqrt(jnp.mean(res * res, axis=-1, keepdims=True) + EPS)
    own = pl.ds(pl.multiple_of(y * Q, Q), Q)
    tok[me] = (res_s[:, own] * scale * mix_gain).astype(BF)
    pl.semaphore_wait(barrier, len(peers))

    def z_start(buf, ss, rs):
        for k, d in ((2, 4), (3, -4), (0, 1), (1, -1), (4, 2), (5, -2)):
            send(buf.at[z], buf.at[z], ss.at[k], rs.at[k], dev(dz=d))

    def z_finish(buf, ss, rs, first, second):
        def block(d, part=None):
            ref = buf.at[zi(d)]
            return ref if part is None else ref.at[part]

        def pass_on(k, d, to, part=None):
            send(block(d, part), block(d, part), ss.at[k], rs.at[k], dev(dz=to))

        def got(k, d, part=None):
            arrive(block(d, part), ss.at[k], rs.at[k])

        got(2, -4)
        pass_on(6, -4, 4, first)
        got(3, 4)
        pass_on(10, 4, -4, second)
        for k, d, to in ((7, -4, 1), (8, -4, -1), (9, -4, 2), (11, 4, 1), (12, 4, -1), (13, 4, -2)):
            pass_on(k, d, to)
        got(6, 8, first)
        got(10, 8, second)
        pass_on(14, 8, 1)
        pass_on(15, 8, -1)
        for k, d in (
            (0, -1), (1, 1), (4, -2), (5, 2), (7, -5), (8, -3),
            (9, -6), (11, 3), (12, 5), (13, 6), (14, 7), (15, 9),
        ):
            got(k, d)

    z_start(wz, z1s, z1r)
    for i, g in enumerate(groups[1:], 1):
        send(tok.at[me], tok.at[me], toks.at[i], tokr.at[i], dev(dx=g[0], dc=g[1]))
    for copy in loads:
        copy.start()
    own_down.start()
    for k in range(1, NY):
        send(quarter(ed_hbm, yi(k)), dq.at[y], ds_.at[k], dr.at[k], dev(dy=k))

    ids_s[...] = jnp.full_like(ids_s, -1.0)
    ids_s[0:TOPK, 0:SEQ] = ids_v[...].astype(F32)
    rw_s[...] = jnp.zeros_like(rw_s)
    rw_s[0:TOPK, 0:SEQ] = rw_v[...]
    ids, rw = jnp.transpose(ids_s[...])[0:16], jnp.transpose(rw_s[...])[0:16]
    lane = iota((16, 256), 1)
    expert, slot = (lane // 2).astype(F32), lane % 2
    row = iota((16, 256), 0).astype(F32)
    named = jnp.zeros((16, 256), F32)
    weight = jnp.zeros((16, 256), F32)
    for j in range(TOPK):
        hit = ids[:, j : j + 1] == expert
        named = jnp.where(hit, 1.0, named)
        weight = jnp.where(hit, rw[:, j : j + 1], weight)
    low = jnp.min(jnp.where(named > 0.5, row, 99.0), axis=0, keepdims=True)
    high = jnp.max(jnp.where(named > 0.5, row, -1.0), axis=0, keepdims=True)
    second = jnp.where(high > low, high, 99.0)
    table = jnp.where(slot[0:1] == 0, low, second)
    combine = jnp.where(row == table, weight, 0.0)
    comb_hi, comb_lo = split_two(combine)

    k_id = iota((1024, 1), 0)
    k_xc, k_in = k_id // 128, k_id % 128
    k_q, k_pj = k_in // 64, k_in % 64
    k_p, k_j = k_pj // COLS, k_pj % COLS
    target = jnp.where(k_pj < 48, k_p * 256 + k_q * 96 + COLS * k_xc + k_j, -1)
    order_in = jnp.where(iota((1024, 1024), 1) == target, 1.0, 0.0).astype(BF)
    perm_in[...] = order_in

    z_finish(wz, z1s, z1r, (pl.ds(0, 32),), (pl.ds(32, 32),))

    wo_own = wz.at[:, pl.ds(48, 16), :]
    own_wo = pltpu.make_async_copy(wo_own, wo.at[me], local.at[5])
    own_wo.start()
    for i, g in enumerate(groups[1:], 1):
        arrive(tok.at[xc_from(g)], toks.at[i], tokr.at[i])
    tokens = tok[...].reshape(XC * 16, Q)

    pairs = [(g, dy) for dy in range(NY) for g in groups]
    for k in range(NY):
        part = yi(k)
        block = wz[pl.ds(4 * part, 4)].reshape(256, Q)
        psend[part] = dot_t(tokens, block).astype(BF).reshape(XC, 16, 256)
    precv[y, me] = psend[y, me]
    for i, (g, dy) in enumerate(pairs):
        if i == 0:
            continue
        send(
            psend.at[yi(dy), xc_to(g)],
            precv.at[y, me],
            ps.at[i],
            pr.at[i],
            dev(dx=g[0], dc=g[1], dy=dy),
        )
    for dx in range(1, NX):
        send(wo_own, wo.at[me], wos.at[dx], wor.at[dx], dev(dx=dx))
    send(wo_own, wo.at[me], wos.at[0], wor.at[0], dev(dc=1))

    for i, (g, dy) in enumerate(pairs):
        if i:
            arrive(precv.at[yi(-dy), xc_from(g)], ps.at[i], pr.at[i])
    halves = [[], []]
    for e in range(XC):
        total = precv[0, e].astype(F32)
        for k in range(1, NY):
            total = total + precv[k, e].astype(F32)
        total = total.astype(BF)
        halves[0].append(total[:, 0:128])
        halves[1].append(total[:, 128:256])
    stacked = jnp.concatenate(
        [jnp.concatenate(half, axis=1) for half in halves], axis=0
    )
    ordered = dot(stacked, perm_in[...])
    narrow = iota((16, 128), 1) < 64
    proj = []
    for p in range(4):
        a = ordered[0:16, 256 * p : 256 * p + 256]
        b = ordered[16:32, 256 * p : 256 * p + 256]
        b0 = pltpu.roll(b[:, 0:128], 64, 1)
        b1 = pltpu.roll(b[:, 128:256], 64, 1)
        proj.append(
            [a[:, 0:128], jnp.where(narrow, a[:, 128:256], b0), jnp.where(narrow, b0, b1)]
        )
    gates = []
    for h in range(HL):
        lower = lower_all[:, h * HEAD : (h + 1) * HEAD]
        query = proj[0][h] * sigmoid(proj[0][h])
        forget = lower + (1.0 - lower) * sigmoid(proj[1][h])
        for n, values in enumerate((query, forget)):
            tall = jnp.concatenate([values, jnp.zeros((112, 128), F32)], axis=0)
            cols[n, h] = jnp.transpose(tall)
        rows_s[h] = proj[2][h]
        gates.append(proj[3][h] * sigmoid(proj[3][h]))

    loads[0].wait()
    read_s[...] = jnp.zeros_like(read_s)

    def one_head(h, _):
        queries, forgets, values = cols[0, h], cols[1, h], rows_s[h]
        for s in range(SEQ):
            f = forgets[:, s : s + 1]
            q = queries[:, s : s + 1]
            v = values[s : s + 1, :]
            nxt = f * state_v[s, h].astype(F32) + (1.0 - f) * v
            state_o[s, h] = nxt.astype(BF)
            read_s[h, s : s + 1, :] = jnp.sum(q * nxt, axis=0, keepdims=True)
        return 0

    lax.fori_loop(0, HL, one_head, 0)
    store = pltpu.make_async_copy(state_o, new_state_hbm, local.at[6])
    store.start()
    for h in range(HL):
        r = read_s[h]
        r = r * lax.rsqrt(jnp.mean(r * r, axis=-1, keepdims=True) + EPS)
        ho[:, h * HEAD : (h + 1) * HEAD] = (r * head_gain * gates[h]).astype(BF)

    for dx in range(1, NX):
        src = lax.rem(x - dx + NX, NX) * NC + c
        arrive(wo.at[src], wos.at[dx], wor.at[dx])
        send(wo.at[src], wo.at[src], wos.at[NX + dx], wor.at[NX + dx], dev(dc=1))
    other = 1 - c
    arrive(wo.at[x * NC + other], wos.at[0], wor.at[0])
    for dx in range(1, NX):
        src = lax.rem(x - dx + NX, NX) * NC + other
        arrive(wo.at[src], wos.at[NX + dx], wor.at[NX + dx])
    own_wo.wait()
    heads = ho[...]
    for k in (1, 2, 3, 0):
        part = yi(k)
        block = wo[:, pl.ds(4 * part, 4)].reshape(512, Q)
        rsend[part] = dot_t(heads, block).astype(BF)
        if k:
            send(rsend.at[part], rrecv.at[y], rss.at[k], rsr.at[k], dev(dy=k))
    rrecv[y] = rsend[y]
    o_id = iota((512, 1), 0)
    o_xc, o_q, o_j = o_id // 64, (o_id // 16) % 4, o_id % 16
    o_to = jnp.where(o_j < COLS, 96 * o_q + COLS * o_xc + o_j, -1)
    order_out = jnp.where(iota((512, Q), 1) == o_to, 1.0, 0.0).astype(BF)
    for k in range(1, NY):
        arrive(rrecv.at[yi(-k)], rss.at[k], rsr.at[k])
    total = rrecv[0].astype(F32)
    for k in range(1, NY):
        total = total + rrecv[k].astype(F32)
    both = dot(jnp.concatenate(split_two(total), axis=0), order_out)
    after = (res_s[:, own] + (both[0:16] + both[16:32])).astype(BF).astype(F32)
    square = jnp.sum(after * after, axis=-1, keepdims=True)
    ssend[...] = jnp.broadcast_to(square, (16, 128))
    srecv[y] = ssend[...]
    for k in range(1, NY):
        send(ssend, srecv.at[y], sss.at[k], ssr.at[k], dev(dy=k))
    gained = after * ffn_gain
    table_row = jnp.concatenate([table, jnp.zeros((1, 128), F32)], axis=1)
    is_table = iota((16, Q), 0) == SEQ
    for k in range(1, NY):
        arrive(srecv.at[yi(-k)], sss.at[k], ssr.at[k])
    square = srecv[0] + srecv[1] + srecv[2] + srecv[3]
    inverse = lax.rsqrt(square[:, 0:1] * (1.0 / D) + EPS)
    tz[z] = jnp.where(is_table, table_row, gained * inverse).astype(BF)

    z_start(tz, z2s, z2r)
    r_id, l_id = iota((256, 256), 0), iota((256, 256), 1)
    spread = jnp.where((r_id // 16 == l_id // 16) & (l_id % 16 == SEQ), 1.0, 0.0).astype(BF)
    mine = jnp.where(iota((16, 256), 1) == 16 * z + iota((16, 256), 0), 1.0, 0.0).astype(BF)
    same = iota((16, 256), 0) == iota((16, 256), 1) // 16
    token = (iota((16, 256), 1) % 16).astype(F32)
    loads[1].wait()
    loads[2].wait()
    z_finish(tz, z2s, z2r, (slice(None), pl.ds(0, 256)), (slice(None), pl.ds(256, 128)))
    flat = tz[...].reshape(256, Q)
    tables = dot(spread, flat[:, 0:256]).astype(BF)
    wanted = dot_t(mine, tables)
    hit = jnp.where(wanted == token, 1.0, 0.0)
    same_f = jnp.where(same, 1.0, 0.0)
    pick = (hit[:, None, :] * same_f[None, :, :]).reshape(256, 256).astype(BF)
    xsend[...] = dot(pick, flat).astype(BF).reshape(XC, 32, Q)
    xf[y, me] = xsend[me]
    for i, g in enumerate(groups[1:], 1):
        send(xsend.at[xc_to(g)], xf.at[y, me], xs.at[i], xr.at[i], dev(dx=g[0], dc=g[1]))
    for i, g in enumerate(groups):
        chunk = xf.at[y, xc_from(g)]
        if i:
            arrive(chunk, xs.at[i], xr.at[i])
        send(chunk, chunk, ys.at[0, i], yr.at[0, i], dev(dy=1))
        send(chunk, chunk, ys.at[1, i], yr.at[1, i], dev(dy=-1))

    def weights_of(part):
        at = pl.ds(pl.multiple_of(part * Q, Q), Q)
        return wg_v[at, :], wu_v[at, :]

    def add_part(part, sums):
        rows = xf[part].reshape(256, Q)
        a, b = weights_of(part)
        return sums[0] + dot(rows, a), sums[1] + dot(rows, b)

    sums = add_part(y, (jnp.zeros((256, FQ), F32), jnp.zeros((256, FQ), F32)))
    for i, g in enumerate(groups):
        left = xf.at[yi(-1), xc_from(g)]
        right = xf.at[yi(1), xc_from(g)]
        arrive(left, ys.at[0, i], yr.at[0, i])
        if i < 4:
            send(left, left, ys.at[2, i], yr.at[2, i], dev(dy=1))
        arrive(right, ys.at[1, i], yr.at[1, i])
        if i >= 4:
            send(right, right, ys.at[2, i], yr.at[2, i], dev(dy=-1))
    sums = add_part(yi(-1), sums)
    sums = add_part(yi(1), sums)
    for i, g in enumerate(groups):
        arrive(xf.at[yi(2), xc_from(g)], ys.at[2, i], yr.at[2, i])
    gate, up = add_part(yi(2), sums)
    hf[y] = (gate * sigmoid(gate) * up).astype(BF)

    send(hf.at[y], hf.at[y], hs.at[0], hr.at[0], dev(dy=1))
    send(hf.at[y], hf.at[y], hs.at[1], hr.at[1], dev(dy=-1))
    own_down.wait()
    for k in range(1, NY):
        arrive(dq.at[yi(-k)], ds_.at[k], dr.at[k])
    down = dot(hf[y], dq[y])
    top, bottom = pl.ds(0, 128), pl.ds(128, 128)
    left = hf.at[yi(-1)]
    right = hf.at[yi(1)]
    arrive(left, hs.at[0], hr.at[0])
    send(left.at[top], left.at[top], hs.at[2], hr.at[2], dev(dy=1))
    arrive(right, hs.at[1], hr.at[1])
    send(right.at[bottom], right.at[bottom], hs.at[3], hr.at[3], dev(dy=-1))
    down = down + dot(hf[yi(-1)], dq[yi(-1)]) + dot(hf[yi(1)], dq[yi(1)])
    far = hf.at[yi(2)]
    arrive(far.at[top], hs.at[2], hr.at[2])
    arrive(far.at[bottom], hs.at[3], hr.at[3])
    down = down + dot(hf[yi(2)], dq[yi(2)])
    osend[...] = down.astype(BF).reshape(XC, 32, Q)

    orecv[me] = osend[me]
    for i, g in enumerate(groups[1:], 1):
        send(osend.at[xc_to(g)], orecv.at[me], os_.at[i], or_.at[i], dev(dx=g[0], dc=g[1]))
    to_z, to_e = r_id // 16, r_id % 16
    source = (to_e // 2) * 32 + (to_e % 2) * 16 + to_z
    turn = jnp.where(l_id == source, 1.0, 0.0).astype(BF)
    for i, g in enumerate(groups[1:], 1):
        arrive(orecv.at[xc_from(g)], os_.at[i], or_.at[i])
    zsend[...] = dot(turn, orecv[...].reshape(256, Q)).astype(BF).reshape(NZ, 16, Q)
    zrecv[z] = zsend[z]
    for d in (8, 7, 9, 6, 10, 5, 11, 4, 12, 3, 13, 2, 14, 1, 15):
        send(zsend.at[zi(d)], zrecv.at[z], rets.at[d], retr.at[d], dev(dz=d))
    for d in range(1, NZ):
        arrive(zrecv.at[zi(-d)], rets.at[d], retr.at[d])
    back = zrecv[...].reshape(256, Q)
    both = dot(jnp.concatenate([comb_hi, comb_lo], axis=0), back)
    result = (after + (both[0:16] + both[16:32])).astype(BF)
    out_ref[...] = result[0:SEQ, :]
    store.wait()
    for copy in pending:
        copy.wait_send()


def shards(
    residual_in,
    rec_state,
    mix_gain,
    w_query,
    w_forget,
    w_input,
    w_gate,
    lower_bound,
    head_gain,
    w_out,
    ffn_gain,
    route_ids,
    route_weight,
    expert_gate,
    expert_up,
    expert_down,
):
    vmem = pl.BlockSpec(memory_space=pltpu.VMEM)
    hbm = pl.BlockSpec(memory_space=pl.ANY)
    dma = pltpu.SemaphoreType.DMA
    out = pl.pallas_call(
        kernel,
        out_shape=(
            jax.ShapeDtypeStruct((SEQ, Q), BF),
            jax.ShapeDtypeStruct(rec_state.shape, BF),
        ),
        in_specs=[hbm] * 16,
        out_specs=(vmem, hbm),
        scratch_shapes=[
            pltpu.VMEM((SEQ, D), BF),
            pltpu.VMEM((5, COLS, Q), BF),
            pltpu.VMEM((64, Q), F32),
            pltpu.VMEM((D,), F32),
            pltpu.VMEM((Q,), F32),
            pltpu.VMEM((HEAD,), F32),
            pltpu.VMEM((D,), F32),
            pltpu.VMEM((TOPK, SEQ), jnp.int32),
            pltpu.VMEM((TOPK, SEQ), F32),
            pltpu.VMEM((NZ, 64, Q), BF),
            pltpu.VMEM((XC, NZ, 16, Q), BF),
            pltpu.VMEM((XC, 16, Q), BF),
            pltpu.VMEM((NY, XC, 16, 256), BF),
            pltpu.VMEM((NY, XC, 16, 256), BF),
            pltpu.VMEM((1024, 1024), BF),
            pltpu.VMEM((SEQ, HL, HEAD, HEAD), BF),
            pltpu.VMEM((SEQ, HL, HEAD, HEAD), BF),
            pltpu.VMEM((2, HL, HEAD, 128), F32),
            pltpu.VMEM((HL, 16, HEAD), F32),
            pltpu.VMEM((HL, 16, HEAD), F32),
            pltpu.VMEM((16, Q), BF),
            pltpu.VMEM((NY, 16, 512), BF),
            pltpu.VMEM((NY, 16, 512), BF),
            pltpu.VMEM((16, 128), F32),
            pltpu.VMEM((NY, 16, 128), F32),
            pltpu.VMEM((16, D), F32),
            pltpu.VMEM((128, 128), F32),
            pltpu.VMEM((128, 128), F32),
            pltpu.VMEM((NZ, 16, Q), BF),
            pltpu.VMEM((XC, 32, Q), BF),
            pltpu.VMEM((NY, XC, 32, Q), BF),
            pltpu.VMEM((NY, 256, FQ), BF),
            pltpu.VMEM((NY, FQ, Q), BF),
            pltpu.VMEM((D, FQ), BF),
            pltpu.VMEM((D, FQ), BF),
            pltpu.VMEM((XC, 32, Q), BF),
            pltpu.VMEM((XC, 32, Q), BF),
            pltpu.VMEM((NZ, 16, Q), BF),
            pltpu.VMEM((NZ, 16, Q), BF),
        ]
        + [
            dma((n,))
            for n in (16, 16, 8, 8, 32, 32, 8, 8, 4, 4, 4, 4, 16, 16, 8, 8)
        ]
        + [dma((3, 8)), dma((3, 8))]
        + [dma((n,)) for n in (4, 4, 4, 4, 8, 8, 16, 16, 20)],
        compiler_params=pltpu.CompilerParams(
            collective_id=0, has_side_effects=True, vmem_limit_bytes=63 * 1024 * 1024
        ),
    )(
        residual_in,
        w_query.T,
        w_forget.T,
        w_input.T,
        w_gate.T,
        w_out.T,
        mix_gain,
        lower_bound,
        head_gain,
        ffn_gain,
        route_ids.T,
        route_weight.T,
        rec_state,
        expert_gate.reshape(D, FQ),
        expert_up.reshape(D, FQ),
        expert_down.reshape(FQ, D),
    )
    return out


def solution(mesh):
    split = Mesh(mesh.devices.reshape(NZ, NX, NC, NY), ("ep_0", "ep_1", "ep_2", "tp"))
    in_specs = (
        P(EP, None),
        P(EP, "tp", None, None),
        P(),
        P("tp", EP),
        P("tp", EP),
        P("tp", EP),
        P("tp", EP),
        P("tp"),
        P(),
        P("tp", EP),
        P(),
        P(EP, None),
        P(EP, None),
        P(EP, None, "tp"),
        P(EP, None, "tp"),
        P(EP, "tp", None),
    )
    out_specs = (P(EP, "tp"), P(EP, "tp", None, None))
    return jax.shard_map(
        shards, mesh=split, in_specs=in_specs, out_specs=out_specs, check_vma=False
    )
```

```python
import jax
import jax.numpy as jnp
from jax import lax
from jax.experimental import pallas as pl
from jax.experimental.pallas import tpu as pltpu
from jax.sharding import Mesh
from jax.sharding import PartitionSpec as P

EP = ("ep_0", "ep_1", "ep_2")
EPS = 1e-06
BF = jnp.bfloat16
F32 = jnp.float32
NZ, NX, NC, NY = 16, 4, 2, 4
XC = NX * NC
D, Q, SEQ, HEAD, HL, FQ, TOPK = 1536, 384, 15, 128, 3, 128, 6
COLS = 12


def dot(a, b):
    return lax.dot_general(a, b, (((1,), (0,)), ((), ())), preferred_element_type=F32)


def dot_t(a, b):
    return lax.dot_general(a, b, (((1,), (1,)), ((), ())), preferred_element_type=F32)


def iota(shape, dim):
    return lax.broadcasted_iota(jnp.int32, shape, dim)


def split_two(x):
    hi = x.astype(BF)
    return hi, (x - hi.astype(F32)).astype(BF)


def sigmoid(x):
    return 1.0 / (1.0 + jnp.exp(-x))


def kernel(
    res_hbm,
    wq_hbm,
    wf_hbm,
    wi_hbm,
    wg_hbm,
    wo_hbm,
    mix_gain_hbm,
    lower_hbm,
    head_gain_hbm,
    ffn_gain_hbm,
    ids_hbm,
    rw_hbm,
    state_hbm,
    eg_hbm,
    eu_hbm,
    ed_hbm,
    out_ref,
    new_state_hbm,
    res_ref,
    w_v,
    w_all,
    mix_gain_v,
    lower_v,
    head_gain_v,
    ffn_gain_v,
    ids_v,
    rw_v,
    wz,
    wo,
    tok,
    hall,
    order_out,
    psend,
    precv,
    perm_in,
    state_v,
    state_o,
    cols,
    rows_s,
    read_s,
    ho,
    rsend,
    rrecv,
    ssend,
    srecv,
    res_s,
    ids_s,
    rw_s,
    tz,
    xsend,
    xf,
    hf,
    dq,
    wg_v,
    wu_v,
    osend,
    orecv,
    zsend,
    zrecv,
    z1s,
    z1r,
    toks,
    tokr,
    ps,
    pr,
    hgs,
    hgr,
    z3s,
    z3r,
    rss,
    rsr,
    sss,
    ssr,
    z2s,
    z2r,
    xs,
    xr,
    ys,
    yr,
    hs,
    hr,
    ds_,
    dr,
    os_,
    or_,
    rets,
    retr,
    local,
):
    z = lax.axis_index("ep_0")
    x = lax.axis_index("ep_1")
    c = lax.axis_index("ep_2")
    y = lax.axis_index("tp")
    me = x * NC + c
    pending = []

    def dev(dz=0, dx=0, dc=0, dy=0):
        return {
            "ep_0": lax.rem(z + dz + NZ, NZ),
            "ep_1": lax.rem(x + dx + NX, NX),
            "ep_2": lax.rem(c + dc + NC, NC),
            "tp": lax.rem(y + dy + NY, NY),
        }

    def send(src, dst, ss, rs, to):
        copy = pltpu.make_async_remote_copy(
            src_ref=src,
            dst_ref=dst,
            send_sem=ss,
            recv_sem=rs,
            device_id=to,
            device_id_type=pl.DeviceIdType.MESH,
        )
        copy.start()
        pending.append(copy)

    def arrive(dst, ss, rs):
        pltpu.make_async_remote_copy(
            src_ref=dst,
            dst_ref=dst,
            send_sem=ss,
            recv_sem=rs,
            device_id=dev(),
            device_id_type=pl.DeviceIdType.MESH,
        ).wait_recv()

    def zi(d):
        return lax.rem(z + d + NZ, NZ)

    def yi(d):
        return lax.rem(y + d + NY, NY)

    groups = [(dx, dc) for dx in range(NX) for dc in range(NC)]

    def xc_to(g):
        return lax.rem(x + g[0], NX) * NC + lax.rem(c + g[1], NC)

    def xc_from(g):
        return lax.rem(x - g[0] + NX, NX) * NC + lax.rem(c - g[1] + NC, NC)

    loads = [
        pltpu.make_async_copy(state_hbm, state_v, local.at[0]),
        pltpu.make_async_copy(eg_hbm, wg_v, local.at[1]),
        pltpu.make_async_copy(eu_hbm, wu_v, local.at[2]),
    ]
    early = [
        (wq_hbm, w_v.at[0]),
        (wf_hbm, w_v.at[1]),
        (wi_hbm, w_v.at[2]),
        (wg_hbm, w_v.at[3]),
        (wo_hbm, w_v.at[4]),
        (res_hbm, res_ref),
        (mix_gain_hbm, mix_gain_v),
        (lower_hbm, lower_v),
        (head_gain_hbm, head_gain_v),
        (ffn_gain_hbm, ffn_gain_v),
        (ids_hbm, ids_v),
        (rw_hbm, rw_v),
    ]
    early = [
        pltpu.make_async_copy(src, dst, local.at[8 + n])
        for n, (src, dst) in enumerate(early)
    ]
    for copy in early:
        copy.start()

    def quarter(ref, part):
        return ref.at[:, pl.ds(pl.multiple_of(part * Q, Q), Q)]

    own_down = pltpu.make_async_copy(quarter(ed_hbm, y), dq.at[y], local.at[3])

    barrier = pltpu.get_barrier_semaphore()
    peers = [dict(dz=d) for d in (1, -1, 4, -4)]
    for g in groups:
        for dy in range(NY):
            if g != (0, 0) or dy:
                peers.append(dict(dx=g[0], dc=g[1], dy=dy))
    for p in peers:
        pl.semaphore_signal(
            barrier, inc=1, device_id=dev(**p), device_id_type=pl.DeviceIdType.MESH
        )

    res_s[...] = jnp.zeros_like(res_s)
    w_all[...] = jnp.zeros_like(w_all)
    for copy in early:
        copy.wait()
    for n in range(5):
        w_all[n * COLS : (n + 1) * COLS, :] = w_v[n].astype(F32)
    wz[:, 48:64, :] = jnp.zeros((NZ, 16, Q), BF)
    wz[z, 0:48, :] = w_all[0:48, :].astype(BF)
    res_s[0:SEQ, :] = res_ref[...].astype(F32)
    res = res_s[...]
    mix_gain = mix_gain_v[pl.ds(pl.multiple_of(y * Q, Q), Q)].reshape(1, Q)
    ffn_gain = ffn_gain_v[pl.ds(pl.multiple_of(y * Q, Q), Q)].reshape(1, Q)
    lower_all = lower_v[...].reshape(1, Q)
    head_gain = head_gain_v[...].reshape(1, HEAD)
    scale = lax.rsqrt(jnp.mean(res * res, axis=-1, keepdims=True) + EPS)
    own = pl.ds(pl.multiple_of(y * Q, Q), Q)
    tok[me] = (res_s[:, own] * scale * mix_gain).astype(BF)
    pl.semaphore_wait(barrier, len(peers))

    def z_ways(view, ss, rs):
        def pass_on(k, d, to, half=None):
            send(view(d, half), view(d, half), ss.at[k], rs.at[k], dev(dz=to))

        def got(k, d, half=None):
            arrive(view(d, half), ss.at[k], rs.at[k])

        return pass_on, got

    def lean_start(ways):
        pass_on, _ = ways
        for k, to in ((2, 4), (3, -4), (0, 1), (1, -1)):
            pass_on(k, 0, to)

    def lean_middle(ways):
        pass_on, got = ways
        got(0, -1)
        pass_on(4, -1, 1)
        got(1, 1)
        pass_on(5, 1, -1)
        got(2, -4)
        pass_on(6, -4, 4, 0)
        got(3, 4)
        pass_on(10, 4, -4, 1)
        for k, d, to in ((7, -4, 1), (12, 4, -1), (8, -4, -1), (11, 4, 1)):
            pass_on(k, d, to)
        got(7, -5)
        pass_on(9, -5, 1)
        got(12, 5)
        pass_on(13, 5, -1)

    def lean_last(ways):
        pass_on, got = ways
        got(6, 8, 0)
        got(10, 8, 1)
        pass_on(14, 8, 1)
        pass_on(15, 8, -1)

    def lean_rest(ways):
        _, got = ways
        for k, d in ((4, -2), (5, 2), (8, -3), (9, -6), (11, 3), (13, 6), (14, 7), (15, 9)):
            got(k, d)

    def quick_start(ways):
        pass_on, _ = ways
        for k, to in ((6, 6), (7, -6), (4, 4), (5, -4), (2, 2), (3, -2), (0, 1), (1, -1)):
            pass_on(k, 0, to)

    def quick_finish(ways):
        pass_on, got = ways
        got(4, -4)
        pass_on(8, -4, -1)
        got(5, 4)
        pass_on(9, 4, 1)
        got(6, -6)
        pass_on(10, -6, 2, 0)
        pass_on(12, -6, 1)
        pass_on(13, -6, -1)
        got(7, 6)
        pass_on(11, 6, -2, 1)
        pass_on(14, 6, -1)
        pass_on(15, 6, 1)
        for k, d in ((0, -1), (1, 1), (2, -2), (3, 2), (8, -3), (9, 3), (12, -7), (13, -5), (14, 7), (15, 5)):
            got(k, d)
        got(10, 8, 0)
        got(11, 8, 1)

    def lanes_of(buf):
        def view(d, half):
            ref = buf.at[zi(d)]
            if half is None:
                return ref
            return ref.at[:, pl.ds(0, 256)] if half == 0 else ref.at[:, pl.ds(256, 128)]

        return view

    def rows_of(d, half):
        first, count = ((0, 48), (0, 32), (32, 16))[0 if half is None else half + 1]
        return wz.at[zi(d), pl.ds(first, count)]

    in_ways = z_ways(rows_of, z1s, z1r)
    out_ways = z_ways(lanes_of(wo), z3s, z3r)
    tok_ways = z_ways(lanes_of(tz), z2s, z2r)
    lean_start(in_ways)
    for i, g in enumerate(groups[1:], 1):
        send(tok.at[me], tok.at[me], toks.at[i], tokr.at[i], dev(dx=g[0], dc=g[1]))
    for copy in loads:
        copy.start()
    own_down.start()
    for k in range(1, NY):
        send(quarter(ed_hbm, yi(k)), dq.at[y], ds_.at[k], dr.at[k], dev(dy=k))

    ids_s[...] = jnp.full_like(ids_s, -1.0)
    ids_s[0:TOPK, 0:SEQ] = ids_v[...].astype(F32)
    rw_s[...] = jnp.zeros_like(rw_s)
    rw_s[0:TOPK, 0:SEQ] = rw_v[...]
    ids, rw = jnp.transpose(ids_s[...])[0:16], jnp.transpose(rw_s[...])[0:16]
    lane = iota((16, 256), 1)
    expert, slot = (lane // 2).astype(F32), lane % 2
    row = iota((16, 256), 0).astype(F32)
    named = jnp.zeros((16, 256), F32)
    weight = jnp.zeros((16, 256), F32)
    for j in range(TOPK):
        hit = ids[:, j : j + 1] == expert
        named = jnp.where(hit, 1.0, named)
        weight = jnp.where(hit, rw[:, j : j + 1], weight)
    low = jnp.min(jnp.where(named > 0.5, row, 99.0), axis=0, keepdims=True)
    high = jnp.max(jnp.where(named > 0.5, row, -1.0), axis=0, keepdims=True)
    second = jnp.where(high > low, high, 99.0)
    table = jnp.where(slot[0:1] == 0, low, second)
    combine = jnp.where(row == table, weight, 0.0)
    comb_hi, comb_lo = split_two(combine)

    table_row = jnp.concatenate([table, jnp.zeros((1, 128), F32)], axis=1)
    wo[z] = jnp.where(iota((16, Q), 0) == COLS, table_row, w_all[48:64, :]).astype(BF)
    lean_start(out_ways)

    k_id = iota((1024, 1), 0)
    k_xc, k_in = k_id // 128, k_id % 128
    k_q, k_pj = k_in // 64, k_in % 64
    k_p, k_j = k_pj // COLS, k_pj % COLS
    target = jnp.where(k_pj < 48, k_p * 256 + k_q * 96 + COLS * k_xc + k_j, -1)
    order_in = jnp.where(iota((1024, 1024), 1) == target, 1.0, 0.0).astype(BF)
    perm_in[...] = order_in
    o_id = iota((1024, 1), 0)
    o_xc, o_half, o_q, o_j = o_id // 128, (o_id // 64) % 2, (o_id // 16) % 4, o_id % 16
    o_ok = (o_j < COLS) & (o_half == lax.rem(y, 2))
    o_to = jnp.where(o_ok, 96 * o_q + COLS * o_xc + o_j, -1)
    order_out[...] = jnp.where(iota((1024, Q), 1) == o_to, 1.0, 0.0).astype(BF)

    lean_middle(in_ways)
    lean_middle(out_ways)
    lean_last(in_ways)
    lean_rest(in_ways)

    for i, g in enumerate(groups[1:], 1):
        arrive(tok.at[xc_from(g)], toks.at[i], tokr.at[i])
    tokens = tok[...].reshape(XC * 16, Q)

    pairs = [(g, dy) for dy in range(NY) for g in groups]
    for k in range(NY):
        part = yi(k)
        block = wz[pl.ds(4 * part, 4)].reshape(256, Q)
        psend[part] = dot_t(tokens, block).astype(BF).reshape(XC, 16, 256)
    precv[y, me] = psend[y, me]
    for i, (g, dy) in enumerate(pairs):
        if i == 0:
            continue
        send(
            psend.at[yi(dy), xc_to(g)],
            precv.at[y, me],
            ps.at[i],
            pr.at[i],
            dev(dx=g[0], dc=g[1], dy=dy),
        )
    lean_last(out_ways)

    for i, (g, dy) in enumerate(pairs):
        if i:
            arrive(precv.at[yi(-dy), xc_from(g)], ps.at[i], pr.at[i])
    halves = [[], []]
    for e in range(XC):
        total = precv[0, e].astype(F32)
        for k in range(1, NY):
            total = total + precv[k, e].astype(F32)
        total = total.astype(BF)
        halves[0].append(total[:, 0:128])
        halves[1].append(total[:, 128:256])
    stacked = jnp.concatenate(
        [jnp.concatenate(half, axis=1) for half in halves], axis=0
    )
    ordered = dot(stacked, perm_in[...])
    narrow = iota((16, 128), 1) < 64
    proj = []
    for p in range(4):
        a = ordered[0:16, 256 * p : 256 * p + 256]
        b = ordered[16:32, 256 * p : 256 * p + 256]
        b0 = pltpu.roll(b[:, 0:128], 64, 1)
        b1 = pltpu.roll(b[:, 128:256], 64, 1)
        proj.append(
            [a[:, 0:128], jnp.where(narrow, a[:, 128:256], b0), jnp.where(narrow, b0, b1)]
        )
    gates = []
    for h in range(HL):
        lower = lower_all[:, h * HEAD : (h + 1) * HEAD]
        query = proj[0][h] * sigmoid(proj[0][h])
        forget = lower + (1.0 - lower) * sigmoid(proj[1][h])
        for n, values in enumerate((query, forget)):
            tall = jnp.concatenate([values, jnp.zeros((112, 128), F32)], axis=0)
            cols[n, h] = jnp.transpose(tall)
        rows_s[h] = proj[2][h]
        gates.append(proj[3][h] * sigmoid(proj[3][h]))

    loads[0].wait()
    read_s[...] = jnp.zeros_like(read_s)

    def one_head(h, _):
        queries, forgets, values = cols[0, h], cols[1, h], rows_s[h]
        for s in range(SEQ):
            f = forgets[:, s : s + 1]
            q = queries[:, s : s + 1]
            v = values[s : s + 1, :]
            nxt = f * state_v[s, h].astype(F32) + (1.0 - f) * v
            state_o[s, h] = nxt.astype(BF)
            read_s[h, s : s + 1, :] = jnp.sum(q * nxt, axis=0, keepdims=True)
        return 0

    lax.fori_loop(0, HL, one_head, 0)
    store = pltpu.make_async_copy(state_o, new_state_hbm, local.at[6])
    store.start()
    for h in range(HL):
        r = read_s[h]
        r = r * lax.rsqrt(jnp.mean(r * r, axis=-1, keepdims=True) + EPS)
        ho[:, h * HEAD : (h + 1) * HEAD] = (r * head_gain * gates[h]).astype(BF)

    hall[me] = ho[...]
    for i, g in enumerate(groups[1:], 1):
        send(hall.at[me], hall.at[me], hgs.at[i], hgr.at[i], dev(dx=g[0], dc=g[1]))
    lean_rest(out_ways)
    for i, g in enumerate(groups[1:], 1):
        arrive(hall.at[xc_from(g)], hgs.at[i], hgr.at[i])
    mixed = dot_t(hall[...].reshape(128, Q), wo[...].reshape(256, Q)).astype(BF)
    for h in range(2):
        rsend[h] = mixed[:, 128 * h : 128 * h + 128].reshape(XC, 16, 128)
    rrecv[y, me] = rsend[y // 2, me]
    for i, (g, dy) in enumerate(pairs):
        if i:
            send(
                rsend.at[yi(dy) // 2, xc_to(g)],
                rrecv.at[y, me],
                rss.at[i],
                rsr.at[i],
                dev(dx=g[0], dc=g[1], dy=dy),
            )
    for i, (g, dy) in enumerate(pairs):
        if i:
            arrive(rrecv.at[yi(-dy), xc_from(g)], rss.at[i], rsr.at[i])
    sums = []
    for e in range(XC):
        total = rrecv[0, e].astype(F32)
        for k in range(1, NY):
            total = total + rrecv[k, e].astype(F32)
        sums.append(total)
    total = jnp.concatenate(sums, axis=1)
    both = dot(jnp.concatenate(split_two(total), axis=0), order_out[...])
    after = (res_s[:, own] + (both[0:16] + both[16:32])).astype(BF).astype(F32)
    square = jnp.sum(after * after, axis=-1, keepdims=True)
    ssend[...] = jnp.broadcast_to(square, (16, 128))
    srecv[y] = ssend[...]
    for k in range(1, NY):
        send(ssend, srecv.at[y], sss.at[k], ssr.at[k], dev(dy=k))
    gained = after * ffn_gain
    for k in range(1, NY):
        arrive(srecv.at[yi(-k)], sss.at[k], ssr.at[k])
    square = srecv[0] + srecv[1] + srecv[2] + srecv[3]
    inverse = lax.rsqrt(square[:, 0:1] * (1.0 / D) + EPS)
    tz[z] = (gained * inverse).astype(BF)

    quick_start(tok_ways)
    r_id, l_id = iota((256, 256), 0), iota((256, 256), 1)
    spread = jnp.where((r_id // 16 == l_id // 16) & (l_id % 16 == COLS), 1.0, 0.0).astype(BF)
    mine = jnp.where(iota((16, 256), 1) == 16 * z + iota((16, 256), 0), 1.0, 0.0).astype(BF)
    same = iota((16, 256), 0) == iota((16, 256), 1) // 16
    token = (iota((16, 256), 1) % 16).astype(F32)
    loads[1].wait()
    loads[2].wait()
    tables = dot(spread, wo[...].reshape(256, Q)[:, 0:256]).astype(BF)
    wanted = dot_t(mine, tables)
    hit = jnp.where(wanted == token, 1.0, 0.0)
    same_f = jnp.where(same, 1.0, 0.0)
    pick = (hit[:, None, :] * same_f[None, :, :]).reshape(256, 256).astype(BF)
    quick_finish(tok_ways)
    flat = tz[...].reshape(256, Q)
    xsend[...] = dot(pick, flat).astype(BF).reshape(XC, 32, Q)
    xf[y, me] = xsend[me]
    for i, g in enumerate(groups[1:], 1):
        send(xsend.at[xc_to(g)], xf.at[y, me], xs.at[i], xr.at[i], dev(dx=g[0], dc=g[1]))
    for i, g in enumerate(groups):
        chunk = xf.at[y, xc_from(g)]
        if i:
            arrive(chunk, xs.at[i], xr.at[i])
        send(chunk, chunk, ys.at[0, i], yr.at[0, i], dev(dy=1))
        send(chunk, chunk, ys.at[1, i], yr.at[1, i], dev(dy=-1))

    def weights_of(part):
        at = pl.ds(pl.multiple_of(part * Q, Q), Q)
        return wg_v[at, :], wu_v[at, :]

    def add_part(part, sums):
        rows = xf[part].reshape(256, Q)
        a, b = weights_of(part)
        return sums[0] + dot(rows, a), sums[1] + dot(rows, b)

    sums = add_part(y, (jnp.zeros((256, FQ), F32), jnp.zeros((256, FQ), F32)))
    for i, g in enumerate(groups):
        left = xf.at[yi(-1), xc_from(g)]
        right = xf.at[yi(1), xc_from(g)]
        arrive(left, ys.at[0, i], yr.at[0, i])
        if i < 4:
            send(left, left, ys.at[2, i], yr.at[2, i], dev(dy=1))
        arrive(right, ys.at[1, i], yr.at[1, i])
        if i >= 4:
            send(right, right, ys.at[2, i], yr.at[2, i], dev(dy=-1))
    sums = add_part(yi(-1), sums)
    sums = add_part(yi(1), sums)
    for i, g in enumerate(groups):
        arrive(xf.at[yi(2), xc_from(g)], ys.at[2, i], yr.at[2, i])
    gate, up = add_part(yi(2), sums)
    hf[y] = (gate * sigmoid(gate) * up).astype(BF)

    send(hf.at[y], hf.at[y], hs.at[0], hr.at[0], dev(dy=1))
    send(hf.at[y], hf.at[y], hs.at[1], hr.at[1], dev(dy=-1))
    own_down.wait()
    for k in range(1, NY):
        arrive(dq.at[yi(-k)], ds_.at[k], dr.at[k])
    down = dot(hf[y], dq[y])
    top, bottom = pl.ds(0, 128), pl.ds(128, 128)
    left = hf.at[yi(-1)]
    right = hf.at[yi(1)]
    arrive(left, hs.at[0], hr.at[0])
    send(left.at[top], left.at[top], hs.at[2], hr.at[2], dev(dy=1))
    arrive(right, hs.at[1], hr.at[1])
    send(right.at[bottom], right.at[bottom], hs.at[3], hr.at[3], dev(dy=-1))
    down = down + dot(hf[yi(-1)], dq[yi(-1)]) + dot(hf[yi(1)], dq[yi(1)])
    far = hf.at[yi(2)]
    arrive(far.at[top], hs.at[2], hr.at[2])
    arrive(far.at[bottom], hs.at[3], hr.at[3])
    down = down + dot(hf[yi(2)], dq[yi(2)])
    osend[...] = down.astype(BF).reshape(XC, 32, Q)

    orecv[me] = osend[me]
    for i, g in enumerate(groups[1:], 1):
        send(osend.at[xc_to(g)], orecv.at[me], os_.at[i], or_.at[i], dev(dx=g[0], dc=g[1]))
    to_z, to_e = r_id // 16, r_id % 16
    source = (to_e // 2) * 32 + (to_e % 2) * 16 + to_z
    turn = jnp.where(l_id == source, 1.0, 0.0).astype(BF)
    for i, g in enumerate(groups[1:], 1):
        arrive(orecv.at[xc_from(g)], os_.at[i], or_.at[i])
    zsend[...] = dot(turn, orecv[...].reshape(256, Q)).astype(BF).reshape(NZ, 16, Q)
    zrecv[z] = zsend[z]
    for d in (8, 7, 9, 6, 10, 5, 11, 4, 12, 3, 13, 2, 14, 1, 15):
        send(zsend.at[zi(d)], zrecv.at[z], rets.at[d], retr.at[d], dev(dz=d))
    for d in range(1, NZ):
        arrive(zrecv.at[zi(-d)], rets.at[d], retr.at[d])
    back = zrecv[...].reshape(256, Q)
    both = dot(jnp.concatenate([comb_hi, comb_lo], axis=0), back)
    result = (after + (both[0:16] + both[16:32])).astype(BF)
    out_ref[...] = result[0:SEQ, :]
    store.wait()
    for copy in pending:
        copy.wait_send()


def shards(
    residual_in,
    rec_state,
    mix_gain,
    w_query,
    w_forget,
    w_input,
    w_gate,
    lower_bound,
    head_gain,
    w_out,
    ffn_gain,
    route_ids,
    route_weight,
    expert_gate,
    expert_up,
    expert_down,
):
    vmem = pl.BlockSpec(memory_space=pltpu.VMEM)
    hbm = pl.BlockSpec(memory_space=pltpu.HBM)
    anywhere = pl.BlockSpec(memory_space=pl.ANY)
    dma = pltpu.SemaphoreType.DMA
    out = pl.pallas_call(
        kernel,
        out_shape=(
            jax.ShapeDtypeStruct((SEQ, Q), BF),
            jax.ShapeDtypeStruct(rec_state.shape, BF),
        ),
        in_specs=[hbm] * 16,
        out_specs=(vmem, anywhere),
        scratch_shapes=[
            pltpu.VMEM((SEQ, D), BF),
            pltpu.VMEM((5, COLS, Q), BF),
            pltpu.VMEM((64, Q), F32),
            pltpu.VMEM((D,), F32),
            pltpu.VMEM((Q,), F32),
            pltpu.VMEM((HEAD,), F32),
            pltpu.VMEM((D,), F32),
            pltpu.VMEM((TOPK, SEQ), jnp.int32),
            pltpu.VMEM((TOPK, SEQ), F32),
            pltpu.VMEM((NZ, 64, Q), BF),
            pltpu.VMEM((NZ, 16, Q), BF),
            pltpu.VMEM((XC, 16, Q), BF),
            pltpu.VMEM((XC, 16, Q), BF),
            pltpu.VMEM((1024, Q), BF),
            pltpu.VMEM((NY, XC, 16, 256), BF),
            pltpu.VMEM((NY, XC, 16, 256), BF),
            pltpu.VMEM((1024, 1024), BF),
            pltpu.VMEM((SEQ, HL, HEAD, HEAD), BF),
            pltpu.VMEM((SEQ, HL, HEAD, HEAD), BF),
            pltpu.VMEM((2, HL, HEAD, 128), F32),
            pltpu.VMEM((HL, 16, HEAD), F32),
            pltpu.VMEM((HL, 16, HEAD), F32),
            pltpu.VMEM((16, Q), BF),
            pltpu.VMEM((2, XC, 16, 128), BF),
            pltpu.VMEM((NY, XC, 16, 128), BF),
            pltpu.VMEM((16, 128), F32),
            pltpu.VMEM((NY, 16, 128), F32),
            pltpu.VMEM((16, D), F32),
            pltpu.VMEM((128, 128), F32),
            pltpu.VMEM((128, 128), F32),
            pltpu.VMEM((NZ, 16, Q), BF),
            pltpu.VMEM((XC, 32, Q), BF),
            pltpu.VMEM((NY, XC, 32, Q), BF),
            pltpu.VMEM((NY, 256, FQ), BF),
            pltpu.VMEM((NY, FQ, Q), BF),
            pltpu.VMEM((D, FQ), BF),
            pltpu.VMEM((D, FQ), BF),
            pltpu.VMEM((XC, 32, Q), BF),
            pltpu.VMEM((XC, 32, Q), BF),
            pltpu.VMEM((NZ, 16, Q), BF),
            pltpu.VMEM((NZ, 16, Q), BF),
        ]
        + [
            dma((n,))
            for n in (16, 16, 8, 8, 32, 32, 8, 8, 16, 16, 32, 32, 4, 4, 16, 16, 8, 8)
        ]
        + [dma((3, 8)), dma((3, 8))]
        + [dma((n,)) for n in (4, 4, 4, 4, 8, 8, 16, 16, 20)],
        compiler_params=pltpu.CompilerParams(
            collective_id=0, has_side_effects=True, vmem_limit_bytes=63 * 1024 * 1024
        ),
    )(
        residual_in,
        w_query.T,
        w_forget.T,
        w_input.T,
        w_gate.T,
        w_out.T,
        mix_gain,
        lower_bound,
        head_gain,
        ffn_gain,
        route_ids.T,
        route_weight.T,
        rec_state,
        expert_gate.reshape(D, FQ),
        expert_up.reshape(D, FQ),
        expert_down.reshape(FQ, D),
    )
    return out


def solution(mesh):
    split = Mesh(mesh.devices.reshape(NZ, NX, NC, NY), ("ep_0", "ep_1", "ep_2", "tp"))
    in_specs = (
        P(EP, None),
        P(EP, "tp", None, None),
        P(),
        P("tp", EP),
        P("tp", EP),
        P("tp", EP),
        P("tp", EP),
        P("tp"),
        P(),
        P("tp", EP),
        P(),
        P(EP, None),
        P(EP, None),
        P(EP, None, "tp"),
        P(EP, None, "tp"),
        P(EP, "tp", None),
    )
    out_specs = (P(EP, "tp"), P(EP, "tp", None, None))
    return jax.shard_map(
        shards, mesh=split, in_specs=in_specs, out_specs=out_specs, check_vma=False
    )
```

```python
import jax
import jax.numpy as jnp
from jax import lax
from jax.experimental import pallas as pl
from jax.experimental.pallas import tpu as pltpu
from jax.sharding import Mesh
from jax.sharding import PartitionSpec as P

EP = ("ep_0", "ep_1", "ep_2")
EPS = 1e-06
BF = jnp.bfloat16
F32 = jnp.float32
NZ, NX, NC, NY = 16, 4, 2, 4
XC = NX * NC
D, Q, SEQ, HEAD, HL, FQ, TOPK = 1536, 384, 15, 128, 3, 128, 6
COLS = 12


def dot(a, b):
    return lax.dot_general(a, b, (((1,), (0,)), ((), ())), preferred_element_type=F32)


def dot_t(a, b):
    return lax.dot_general(a, b, (((1,), (1,)), ((), ())), preferred_element_type=F32)


def iota(shape, dim):
    return lax.broadcasted_iota(jnp.int32, shape, dim)


def split_two(x):
    hi = x.astype(BF)
    return hi, (x - hi.astype(F32)).astype(BF)


def sigmoid(x):
    return 1.0 / (1.0 + jnp.exp(-x))


def kernel(
    res_hbm,
    wq_hbm,
    wf_hbm,
    wi_hbm,
    wg_hbm,
    wo_hbm,
    mix_gain_hbm,
    lower_hbm,
    head_gain_hbm,
    ffn_gain_hbm,
    ids_hbm,
    rw_hbm,
    state_hbm,
    eg_hbm,
    eu_hbm,
    ed_hbm,
    out_ref,
    new_state_hbm,
    res_ref,
    w_v,
    w_all,
    mix_gain_v,
    lower_v,
    head_gain_v,
    ffn_gain_v,
    ids_v,
    rw_v,
    wz,
    wo,
    tok,
    hall,
    order_out,
    psend,
    precv,
    perm_in,
    state_v,
    state_o,
    cols,
    rows_s,
    read_s,
    ho,
    rsend,
    rrecv,
    ssend,
    srecv,
    res_s,
    ids_s,
    rw_s,
    tz,
    xsend,
    xf,
    hf,
    dq,
    wg_v,
    wu_v,
    osend,
    orecv,
    zsend,
    zrecv,
    z1s,
    z1r,
    toks,
    tokr,
    ps,
    pr,
    hgs,
    hgr,
    z3s,
    z3r,
    rss,
    rsr,
    sss,
    ssr,
    z2s,
    z2r,
    xs,
    xr,
    ys,
    yr,
    hs,
    hr,
    ds_,
    dr,
    os_,
    or_,
    rets,
    retr,
    local,
):
    z = lax.axis_index("ep_0")
    x = lax.axis_index("ep_1")
    c = lax.axis_index("ep_2")
    y = lax.axis_index("tp")
    me = x * NC + c
    pending = []

    def dev(dz=0, dx=0, dc=0, dy=0):
        return {
            "ep_0": lax.rem(z + dz + NZ, NZ),
            "ep_1": lax.rem(x + dx + NX, NX),
            "ep_2": lax.rem(c + dc + NC, NC),
            "tp": lax.rem(y + dy + NY, NY),
        }

    def send(src, dst, ss, rs, to):
        copy = pltpu.make_async_remote_copy(
            src_ref=src,
            dst_ref=dst,
            send_sem=ss,
            recv_sem=rs,
            device_id=to,
            device_id_type=pl.DeviceIdType.MESH,
        )
        copy.start()
        pending.append(copy)

    def arrive(dst, ss, rs):
        pltpu.make_async_remote_copy(
            src_ref=dst,
            dst_ref=dst,
            send_sem=ss,
            recv_sem=rs,
            device_id=dev(),
            device_id_type=pl.DeviceIdType.MESH,
        ).wait_recv()

    def zi(d):
        return lax.rem(z + d + NZ, NZ)

    def yi(d):
        return lax.rem(y + d + NY, NY)

    groups = [(dx, dc) for dx in range(NX) for dc in range(NC)]

    def xc_to(g):
        return lax.rem(x + g[0], NX) * NC + lax.rem(c + g[1], NC)

    def xc_from(g):
        return lax.rem(x - g[0] + NX, NX) * NC + lax.rem(c - g[1] + NC, NC)

    loads = [
        pltpu.make_async_copy(state_hbm, state_v, local.at[0]),
        pltpu.make_async_copy(eg_hbm, wg_v, local.at[1]),
        pltpu.make_async_copy(eu_hbm, wu_v, local.at[2]),
    ]
    early = [
        (wq_hbm, w_v.at[0]),
        (wf_hbm, w_v.at[1]),
        (wi_hbm, w_v.at[2]),
        (wg_hbm, w_v.at[3]),
        (wo_hbm, w_v.at[4]),
        (res_hbm, res_ref),
        (mix_gain_hbm, mix_gain_v),
        (lower_hbm, lower_v),
        (head_gain_hbm, head_gain_v),
        (ffn_gain_hbm, ffn_gain_v),
        (ids_hbm, ids_v),
        (rw_hbm, rw_v),
    ]
    early = [
        pltpu.make_async_copy(src, dst, local.at[8 + n])
        for n, (src, dst) in enumerate(early)
    ]
    for copy in early:
        copy.start()

    def quarter(ref, part):
        return ref.at[:, pl.ds(pl.multiple_of(part * Q, Q), Q)]

    own_down = pltpu.make_async_copy(quarter(ed_hbm, y), dq.at[y], local.at[3])

    barrier = pltpu.get_barrier_semaphore()
    peers = [dict(dz=d) for d in (1, -1, 4, -4)]
    for g in groups:
        for dy in range(NY):
            if g != (0, 0) or dy:
                peers.append(dict(dx=g[0], dc=g[1], dy=dy))
    for p in peers:
        pl.semaphore_signal(
            barrier, inc=1, device_id=dev(**p), device_id_type=pl.DeviceIdType.MESH
        )

    res_s[...] = jnp.zeros_like(res_s)
    w_all[...] = jnp.zeros_like(w_all)
    for copy in early:
        copy.wait()
    for n in range(5):
        w_all[n * COLS : (n + 1) * COLS, :] = w_v[n].astype(F32)
    wz[:, 48:64, :] = jnp.zeros((NZ, 16, Q), BF)
    wz[z, 0:48, :] = w_all[0:48, :].astype(BF)
    res_s[0:SEQ, :] = res_ref[...].astype(F32)
    res = res_s[...]
    mix_gain = mix_gain_v[pl.ds(pl.multiple_of(y * Q, Q), Q)].reshape(1, Q)
    ffn_gain = ffn_gain_v[pl.ds(pl.multiple_of(y * Q, Q), Q)].reshape(1, Q)
    lower_all = lower_v[...].reshape(1, Q)
    head_gain = head_gain_v[...].reshape(1, HEAD)
    scale = lax.rsqrt(jnp.mean(res * res, axis=-1, keepdims=True) + EPS)
    own = pl.ds(pl.multiple_of(y * Q, Q), Q)
    tok[me] = (res_s[:, own] * scale * mix_gain).astype(BF)
    pl.semaphore_wait(barrier, len(peers))

    def z_ways(view, ss, rs):
        def pass_on(k, d, to, half=None):
            send(view(d, half), view(d, half), ss.at[k], rs.at[k], dev(dz=to))

        def got(k, d, half=None):
            arrive(view(d, half), ss.at[k], rs.at[k])

        return pass_on, got

    def lean_start(ways):
        pass_on, _ = ways
        for k, to in ((2, 4), (3, -4), (0, 1), (1, -1)):
            pass_on(k, 0, to)

    def lean_middle(ways):
        pass_on, got = ways
        got(0, -1)
        pass_on(4, -1, 1)
        got(1, 1)
        pass_on(5, 1, -1)
        got(2, -4)
        pass_on(6, -4, 4, 0)
        got(3, 4)
        pass_on(10, 4, -4, 1)
        for k, d, to in ((7, -4, 1), (12, 4, -1), (8, -4, -1), (11, 4, 1)):
            pass_on(k, d, to)
        got(7, -5)
        pass_on(9, -5, 1)
        got(12, 5)
        pass_on(13, 5, -1)

    def lean_last(ways):
        pass_on, got = ways
        got(6, 8, 0)
        got(10, 8, 1)
        pass_on(14, 8, 1)
        pass_on(15, 8, -1)

    def lean_rest(ways):
        _, got = ways
        for k, d in ((4, -2), (5, 2), (8, -3), (9, -6), (11, 3), (13, 6), (14, 7), (15, 9)):
            got(k, d)

    def quick_start(ways):
        pass_on, _ = ways
        for k, to in ((6, 6), (7, -6), (4, 4), (5, -4), (2, 2), (3, -2), (0, 1), (1, -1)):
            pass_on(k, 0, to)

    def quick_middle(ways):
        pass_on, got = ways
        got(4, -4)
        pass_on(8, -4, -1)
        got(5, 4)
        pass_on(9, 4, 1)
        got(6, -6)
        pass_on(10, -6, 2, 0)
        pass_on(12, -6, 1)
        pass_on(13, -6, -1)
        got(7, 6)
        pass_on(11, 6, -2, 1)
        pass_on(14, 6, -1)
        pass_on(15, 6, 1)

    def quick_rest(ways):
        _, got = ways
        for k, d in ((0, -1), (1, 1), (2, -2), (3, 2), (8, -3), (9, 3), (12, -7), (13, -5), (14, 7), (15, 5)):
            got(k, d)
        got(10, 8, 0)
        got(11, 8, 1)

    def lanes_of(buf):
        def view(d, half):
            ref = buf.at[zi(d)]
            if half is None:
                return ref
            return ref.at[:, pl.ds(0, 256)] if half == 0 else ref.at[:, pl.ds(256, 128)]

        return view

    def rows_of(d, half):
        first, count = ((0, 48), (0, 32), (32, 16))[0 if half is None else half + 1]
        return wz.at[zi(d), pl.ds(first, count)]

    in_ways = z_ways(rows_of, z1s, z1r)
    out_ways = z_ways(lanes_of(wo), z3s, z3r)
    tok_ways = z_ways(lanes_of(tz), z2s, z2r)
    lean_start(in_ways)
    for i, g in enumerate(groups[1:], 1):
        send(tok.at[me], tok.at[me], toks.at[i], tokr.at[i], dev(dx=g[0], dc=g[1]))
    for copy in loads:
        copy.start()
    own_down.start()
    for k in range(1, NY):
        send(quarter(ed_hbm, yi(k)), dq.at[y], ds_.at[k], dr.at[k], dev(dy=k))

    ids_s[...] = jnp.full_like(ids_s, -1.0)
    ids_s[0:TOPK, 0:SEQ] = ids_v[...].astype(F32)
    rw_s[...] = jnp.zeros_like(rw_s)
    rw_s[0:TOPK, 0:SEQ] = rw_v[...]
    ids, rw = jnp.transpose(ids_s[...])[0:16], jnp.transpose(rw_s[...])[0:16]
    lane = iota((16, 256), 1)
    expert, slot = (lane // 2).astype(F32), lane % 2
    row = iota((16, 256), 0).astype(F32)
    named = jnp.zeros((16, 256), F32)
    weight = jnp.zeros((16, 256), F32)
    for j in range(TOPK):
        hit = ids[:, j : j + 1] == expert
        named = jnp.where(hit, 1.0, named)
        weight = jnp.where(hit, rw[:, j : j + 1], weight)
    low = jnp.min(jnp.where(named > 0.5, row, 99.0), axis=0, keepdims=True)
    high = jnp.max(jnp.where(named > 0.5, row, -1.0), axis=0, keepdims=True)
    second = jnp.where(high > low, high, 99.0)
    table = jnp.where(slot[0:1] == 0, low, second)
    combine = jnp.where(row == table, weight, 0.0)
    comb_hi, comb_lo = split_two(combine)

    table_row = jnp.concatenate([table, jnp.zeros((1, 128), F32)], axis=1)
    wo[z] = jnp.where(iota((16, Q), 0) == COLS, table_row, w_all[48:64, :]).astype(BF)

    k_id = iota((1024, 1), 0)
    k_xc, k_in = k_id // 128, k_id % 128
    k_q, k_pj = k_in // 64, k_in % 64
    k_p, k_j = k_pj // COLS, k_pj % COLS
    target = jnp.where(k_pj < 48, k_p * 256 + k_q * 96 + COLS * k_xc + k_j, -1)
    order_in = jnp.where(iota((1024, 1024), 1) == target, 1.0, 0.0).astype(BF)
    perm_in[...] = order_in
    o_id = iota((1024, 1), 0)
    o_xc, o_half, o_q, o_j = o_id // 128, (o_id // 64) % 2, (o_id // 16) % 4, o_id % 16
    o_ok = (o_j < COLS) & (o_half == lax.rem(y, 2))
    o_to = jnp.where(o_ok, 96 * o_q + COLS * o_xc + o_j, -1)
    order_out[...] = jnp.where(iota((1024, Q), 1) == o_to, 1.0, 0.0).astype(BF)

    lean_middle(in_ways)
    lean_last(in_ways)
    quick_start(out_ways)
    lean_rest(in_ways)

    for i, g in enumerate(groups[1:], 1):
        arrive(tok.at[xc_from(g)], toks.at[i], tokr.at[i])
    tokens = tok[...].reshape(XC * 16, Q)

    pairs = [(g, dy) for dy in range(NY) for g in groups]
    for k in range(NY):
        part = yi(k)
        block = wz[pl.ds(4 * part, 4)].reshape(256, Q)
        psend[part] = dot_t(tokens, block).astype(BF).reshape(XC, 16, 256)
    precv[y, me] = psend[y, me]
    for i, (g, dy) in enumerate(pairs):
        if i == 0:
            continue
        send(
            psend.at[yi(dy), xc_to(g)],
            precv.at[y, me],
            ps.at[i],
            pr.at[i],
            dev(dx=g[0], dc=g[1], dy=dy),
        )
    for i, (g, dy) in enumerate(pairs):
        if i:
            arrive(precv.at[yi(-dy), xc_from(g)], ps.at[i], pr.at[i])
    quick_middle(out_ways)
    halves = [[], []]
    for e in range(XC):
        total = precv[0, e].astype(F32)
        for k in range(1, NY):
            total = total + precv[k, e].astype(F32)
        total = total.astype(BF)
        halves[0].append(total[:, 0:128])
        halves[1].append(total[:, 128:256])
    stacked = jnp.concatenate(
        [jnp.concatenate(half, axis=1) for half in halves], axis=0
    )
    ordered = dot(stacked, perm_in[...])
    narrow = iota((16, 128), 1) < 64
    proj = []
    for p in range(4):
        a = ordered[0:16, 256 * p : 256 * p + 256]
        b = ordered[16:32, 256 * p : 256 * p + 256]
        b0 = pltpu.roll(b[:, 0:128], 64, 1)
        b1 = pltpu.roll(b[:, 128:256], 64, 1)
        proj.append(
            [a[:, 0:128], jnp.where(narrow, a[:, 128:256], b0), jnp.where(narrow, b0, b1)]
        )
    gates = []
    for h in range(HL):
        lower = lower_all[:, h * HEAD : (h + 1) * HEAD]
        query = proj[0][h] * sigmoid(proj[0][h])
        forget = lower + (1.0 - lower) * sigmoid(proj[1][h])
        for n, values in enumerate((query, forget)):
            tall = jnp.concatenate([values, jnp.zeros((112, 128), F32)], axis=0)
            cols[n, h] = jnp.transpose(tall)
        rows_s[h] = proj[2][h]
        gates.append(proj[3][h] * sigmoid(proj[3][h]))

    loads[0].wait()
    read_s[...] = jnp.zeros_like(read_s)

    def one_head(h, _):
        queries, forgets, values = cols[0, h], cols[1, h], rows_s[h]
        for s in range(SEQ):
            f = forgets[:, s : s + 1]
            q = queries[:, s : s + 1]
            v = values[s : s + 1, :]
            nxt = f * state_v[s, h].astype(F32) + (1.0 - f) * v
            state_o[s, h] = nxt.astype(BF)
            read_s[h, s : s + 1, :] = jnp.sum(q * nxt, axis=0, keepdims=True)
        return 0

    lax.fori_loop(0, HL, one_head, 0)
    store = pltpu.make_async_copy(state_o, new_state_hbm, local.at[6])
    store.start()
    for h in range(HL):
        r = read_s[h]
        r = r * lax.rsqrt(jnp.mean(r * r, axis=-1, keepdims=True) + EPS)
        ho[:, h * HEAD : (h + 1) * HEAD] = (r * head_gain * gates[h]).astype(BF)

    hall[me] = ho[...]
    for i, g in enumerate(groups[1:], 1):
        send(hall.at[me], hall.at[me], hgs.at[i], hgr.at[i], dev(dx=g[0], dc=g[1]))
    quick_rest(out_ways)
    for i, g in enumerate(groups[1:], 1):
        arrive(hall.at[xc_from(g)], hgs.at[i], hgr.at[i])
    mixed = dot_t(hall[...].reshape(128, Q), wo[...].reshape(256, Q)).astype(BF)
    for h in range(2):
        rsend[h] = mixed[:, 128 * h : 128 * h + 128].reshape(XC, 16, 128)
    rrecv[y, me] = rsend[y // 2, me]
    for i, (g, dy) in enumerate(pairs):
        if i:
            send(
                rsend.at[yi(dy) // 2, xc_to(g)],
                rrecv.at[y, me],
                rss.at[i],
                rsr.at[i],
                dev(dx=g[0], dc=g[1], dy=dy),
            )
    for i, (g, dy) in enumerate(pairs):
        if i:
            arrive(rrecv.at[yi(-dy), xc_from(g)], rss.at[i], rsr.at[i])
    sums = []
    for e in range(XC):
        total = rrecv[0, e].astype(F32)
        for k in range(1, NY):
            total = total + rrecv[k, e].astype(F32)
        sums.append(total)
    total = jnp.concatenate(sums, axis=1)
    both = dot(jnp.concatenate(split_two(total), axis=0), order_out[...])
    after = (res_s[:, own] + (both[0:16] + both[16:32])).astype(BF).astype(F32)
    square = jnp.sum(after * after, axis=-1, keepdims=True)
    ssend[...] = jnp.broadcast_to(square, (16, 128))
    srecv[y] = ssend[...]
    for k in range(1, NY):
        send(ssend, srecv.at[y], sss.at[k], ssr.at[k], dev(dy=k))
    gained = after * ffn_gain
    for k in range(1, NY):
        arrive(srecv.at[yi(-k)], sss.at[k], ssr.at[k])
    square = srecv[0] + srecv[1] + srecv[2] + srecv[3]
    inverse = lax.rsqrt(square[:, 0:1] * (1.0 / D) + EPS)
    tz[z] = (gained * inverse).astype(BF)

    quick_start(tok_ways)
    r_id, l_id = iota((256, 256), 0), iota((256, 256), 1)
    spread = jnp.where((r_id // 16 == l_id // 16) & (l_id % 16 == COLS), 1.0, 0.0).astype(BF)
    mine = jnp.where(iota((16, 256), 1) == 16 * z + iota((16, 256), 0), 1.0, 0.0).astype(BF)
    same = iota((16, 256), 0) == iota((16, 256), 1) // 16
    token = (iota((16, 256), 1) % 16).astype(F32)
    loads[1].wait()
    loads[2].wait()
    tables = dot(spread, wo[...].reshape(256, Q)[:, 0:256]).astype(BF)
    wanted = dot_t(mine, tables)
    hit = jnp.where(wanted == token, 1.0, 0.0)
    same_f = jnp.where(same, 1.0, 0.0)
    pick = (hit[:, None, :] * same_f[None, :, :]).reshape(256, 256).astype(BF)
    quick_middle(tok_ways)
    quick_rest(tok_ways)
    flat = tz[...].reshape(256, Q)
    xsend[...] = dot(pick, flat).astype(BF).reshape(XC, 32, Q)
    xf[y, me] = xsend[me]
    for i, g in enumerate(groups[1:], 1):
        send(xsend.at[xc_to(g)], xf.at[y, me], xs.at[i], xr.at[i], dev(dx=g[0], dc=g[1]))
    for i, g in enumerate(groups):
        chunk = xf.at[y, xc_from(g)]
        if i:
            arrive(chunk, xs.at[i], xr.at[i])
        send(chunk, chunk, ys.at[0, i], yr.at[0, i], dev(dy=1))
        send(chunk, chunk, ys.at[1, i], yr.at[1, i], dev(dy=-1))

    def weights_of(part):
        at = pl.ds(pl.multiple_of(part * Q, Q), Q)
        return wg_v[at, :], wu_v[at, :]

    def add_part(part, sums):
        rows = xf[part].reshape(256, Q)
        a, b = weights_of(part)
        return sums[0] + dot(rows, a), sums[1] + dot(rows, b)

    sums = add_part(y, (jnp.zeros((256, FQ), F32), jnp.zeros((256, FQ), F32)))
    for i, g in enumerate(groups):
        left = xf.at[yi(-1), xc_from(g)]
        right = xf.at[yi(1), xc_from(g)]
        arrive(left, ys.at[0, i], yr.at[0, i])
        if i < 4:
            send(left, left, ys.at[2, i], yr.at[2, i], dev(dy=1))
        arrive(right, ys.at[1, i], yr.at[1, i])
        if i >= 4:
            send(right, right, ys.at[2, i], yr.at[2, i], dev(dy=-1))
    sums = add_part(yi(-1), sums)
    sums = add_part(yi(1), sums)
    for i, g in enumerate(groups):
        arrive(xf.at[yi(2), xc_from(g)], ys.at[2, i], yr.at[2, i])
    gate, up = add_part(yi(2), sums)
    hf[y] = (gate * sigmoid(gate) * up).astype(BF)

    send(hf.at[y], hf.at[y], hs.at[0], hr.at[0], dev(dy=1))
    send(hf.at[y], hf.at[y], hs.at[1], hr.at[1], dev(dy=-1))
    own_down.wait()
    for k in range(1, NY):
        arrive(dq.at[yi(-k)], ds_.at[k], dr.at[k])
    down = dot(hf[y], dq[y])
    top, bottom = pl.ds(0, 128), pl.ds(128, 128)
    left = hf.at[yi(-1)]
    right = hf.at[yi(1)]
    arrive(left, hs.at[0], hr.at[0])
    send(left.at[top], left.at[top], hs.at[2], hr.at[2], dev(dy=1))
    arrive(right, hs.at[1], hr.at[1])
    send(right.at[bottom], right.at[bottom], hs.at[3], hr.at[3], dev(dy=-1))
    down = down + dot(hf[yi(-1)], dq[yi(-1)]) + dot(hf[yi(1)], dq[yi(1)])
    far = hf.at[yi(2)]
    arrive(far.at[top], hs.at[2], hr.at[2])
    arrive(far.at[bottom], hs.at[3], hr.at[3])
    down = down + dot(hf[yi(2)], dq[yi(2)])
    osend[...] = down.astype(BF).reshape(XC, 32, Q)

    orecv[me] = osend[me]
    for i, g in enumerate(groups[1:], 1):
        send(osend.at[xc_to(g)], orecv.at[me], os_.at[i], or_.at[i], dev(dx=g[0], dc=g[1]))
    to_z, to_e = r_id // 16, r_id % 16
    source = (to_e // 2) * 32 + (to_e % 2) * 16 + to_z
    turn = jnp.where(l_id == source, 1.0, 0.0).astype(BF)
    for i, g in enumerate(groups[1:], 1):
        arrive(orecv.at[xc_from(g)], os_.at[i], or_.at[i])
    zsend[...] = dot(turn, orecv[...].reshape(256, Q)).astype(BF).reshape(NZ, 16, Q)
    zrecv[z] = zsend[z]
    for d in (8, 7, 9, 6, 10, 5, 11, 4, 12, 3, 13, 2, 14, 1, 15):
        send(zsend.at[zi(d)], zrecv.at[z], rets.at[d], retr.at[d], dev(dz=d))
    for d in range(1, NZ):
        arrive(zrecv.at[zi(-d)], rets.at[d], retr.at[d])
    back = zrecv[...].reshape(256, Q)
    both = dot(jnp.concatenate([comb_hi, comb_lo], axis=0), back)
    result = (after + (both[0:16] + both[16:32])).astype(BF)
    out_ref[...] = result[0:SEQ, :]
    store.wait()
    for copy in pending:
        copy.wait_send()


def shards(
    residual_in,
    rec_state,
    mix_gain,
    w_query,
    w_forget,
    w_input,
    w_gate,
    lower_bound,
    head_gain,
    w_out,
    ffn_gain,
    route_ids,
    route_weight,
    expert_gate,
    expert_up,
    expert_down,
):
    vmem = pl.BlockSpec(memory_space=pltpu.VMEM)
    hbm = pl.BlockSpec(memory_space=pltpu.HBM)
    anywhere = pl.BlockSpec(memory_space=pl.ANY)
    dma = pltpu.SemaphoreType.DMA
    out = pl.pallas_call(
        kernel,
        out_shape=(
            pltpu.VMEM((SEQ, Q), BF),
            pltpu.VMEM(rec_state.shape, BF),
        ),
        in_specs=[hbm] * 16,
        out_specs=(vmem, anywhere),
        scratch_shapes=[
            pltpu.VMEM((SEQ, D), BF),
            pltpu.VMEM((5, COLS, Q), BF),
            pltpu.VMEM((64, Q), F32),
            pltpu.VMEM((D,), F32),
            pltpu.VMEM((Q,), F32),
            pltpu.VMEM((HEAD,), F32),
            pltpu.VMEM((D,), F32),
            pltpu.VMEM((TOPK, SEQ), jnp.int32),
            pltpu.VMEM((TOPK, SEQ), F32),
            pltpu.VMEM((NZ, 64, Q), BF),
            pltpu.VMEM((NZ, 16, Q), BF),
            pltpu.VMEM((XC, 16, Q), BF),
            pltpu.VMEM((XC, 16, Q), BF),
            pltpu.VMEM((1024, Q), BF),
            pltpu.VMEM((NY, XC, 16, 256), BF),
            pltpu.VMEM((NY, XC, 16, 256), BF),
            pltpu.VMEM((1024, 1024), BF),
            pltpu.VMEM((SEQ, HL, HEAD, HEAD), BF),
            pltpu.VMEM((SEQ, HL, HEAD, HEAD), BF),
            pltpu.VMEM((2, HL, HEAD, 128), F32),
            pltpu.VMEM((HL, 16, HEAD), F32),
            pltpu.VMEM((HL, 16, HEAD), F32),
            pltpu.VMEM((16, Q), BF),
            pltpu.VMEM((2, XC, 16, 128), BF),
            pltpu.VMEM((NY, XC, 16, 128), BF),
            pltpu.VMEM((16, 128), F32),
            pltpu.VMEM((NY, 16, 128), F32),
            pltpu.VMEM((16, D), F32),
            pltpu.VMEM((128, 128), F32),
            pltpu.VMEM((128, 128), F32),
            pltpu.VMEM((NZ, 16, Q), BF),
            pltpu.VMEM((XC, 32, Q), BF),
            pltpu.VMEM((NY, XC, 32, Q), BF),
            pltpu.VMEM((NY, 256, FQ), BF),
            pltpu.VMEM((NY, FQ, Q), BF),
            pltpu.VMEM((D, FQ), BF),
            pltpu.VMEM((D, FQ), BF),
            pltpu.VMEM((XC, 32, Q), BF),
            pltpu.VMEM((XC, 32, Q), BF),
            pltpu.VMEM((NZ, 16, Q), BF),
            pltpu.VMEM((NZ, 16, Q), BF),
        ]
        + [
            dma((n,))
            for n in (16, 16, 8, 8, 32, 32, 8, 8, 16, 16, 32, 32, 4, 4, 16, 16, 8, 8)
        ]
        + [dma((3, 8)), dma((3, 8))]
        + [dma((n,)) for n in (4, 4, 4, 4, 8, 8, 16, 16, 20)],
        compiler_params=pltpu.CompilerParams(
            collective_id=0, has_side_effects=True, vmem_limit_bytes=60 * 1024 * 1024
        ),
    )(
        residual_in,
        w_query.T,
        w_forget.T,
        w_input.T,
        w_gate.T,
        w_out.T,
        mix_gain,
        lower_bound,
        head_gain,
        ffn_gain,
        route_ids.T,
        route_weight.T,
        rec_state,
        expert_gate.reshape(D, FQ),
        expert_up.reshape(D, FQ),
        expert_down.reshape(FQ, D),
    )
    return out


def solution(mesh):
    split = Mesh(mesh.devices.reshape(NZ, NX, NC, NY), ("ep_0", "ep_1", "ep_2", "tp"))
    in_specs = (
        P(EP, None),
        P(EP, "tp", None, None),
        P(),
        P("tp", EP),
        P("tp", EP),
        P("tp", EP),
        P("tp", EP),
        P("tp"),
        P(),
        P("tp", EP),
        P(),
        P(EP, None),
        P(EP, None),
        P(EP, None, "tp"),
        P(EP, None, "tp"),
        P(EP, "tp", None),
    )
    out_specs = (P(EP, "tp"), P(EP, "tp", None, None))
    return jax.shard_map(
        shards, mesh=split, in_specs=in_specs, out_specs=out_specs, check_vma=False
    )
```

```python
import jax
import jax.numpy as jnp
from jax import lax
from jax.experimental import pallas as pl
from jax.experimental.pallas import tpu as pltpu
from jax.sharding import Mesh
from jax.sharding import PartitionSpec as P

EP = ("ep_0", "ep_1", "ep_2")
EPS = 1e-06
BF = jnp.bfloat16
F32 = jnp.float32
NZ, NX, NC, NY = 16, 4, 2, 4
XC = NX * NC
D, Q, SEQ, HEAD, HL, FQ, TOPK = 1536, 384, 15, 128, 3, 128, 6
COLS = 12


def dot(a, b):
    return lax.dot_general(a, b, (((1,), (0,)), ((), ())), preferred_element_type=F32)


def dot_t(a, b):
    return lax.dot_general(a, b, (((1,), (1,)), ((), ())), preferred_element_type=F32)


def iota(shape, dim):
    return lax.broadcasted_iota(jnp.int32, shape, dim)


def split_two(x):
    hi = x.astype(BF)
    return hi, (x - hi.astype(F32)).astype(BF)


def sigmoid(x):
    return 1.0 / (1.0 + jnp.exp(-x))


def kernel(
    res_hbm,
    wq_hbm,
    wf_hbm,
    wi_hbm,
    wg_hbm,
    wo_hbm,
    mix_gain_hbm,
    lower_hbm,
    head_gain_hbm,
    ffn_gain_hbm,
    ids_hbm,
    rw_hbm,
    state_hbm,
    eg_hbm,
    eu_hbm,
    ed_hbm,
    out_ref,
    new_state_hbm,
    res_ref,
    w_v,
    w_all,
    mix_gain_v,
    lower_v,
    head_gain_v,
    ffn_gain_v,
    ids_v,
    rw_v,
    wz,
    wo,
    tok,
    hall,
    order_out,
    psend,
    precv,
    perm_in,
    state_v,
    state_o,
    cols,
    rows_s,
    read_s,
    ho,
    rsend,
    rrecv,
    res_p,
    sum_s,
    res_s,
    ids_s,
    rw_s,
    tz,
    xsend,
    xf,
    hf,
    dq,
    wg_v,
    wu_v,
    osend,
    orecv,
    zsend,
    zrecv,
    z1s,
    z1r,
    toks,
    tokr,
    ps,
    pr,
    hgs,
    hgr,
    z3s,
    z3r,
    rss,
    rsr,
    z2s,
    z2r,
    xs,
    xr,
    ys,
    yr,
    hs,
    hr,
    ds_,
    dr,
    os_,
    or_,
    rets,
    retr,
    local,
):
    z = lax.axis_index("ep_0")
    x = lax.axis_index("ep_1")
    c = lax.axis_index("ep_2")
    y = lax.axis_index("tp")
    me = x * NC + c
    pending = []

    def dev(dz=0, dx=0, dc=0, dy=0):
        return {
            "ep_0": lax.rem(z + dz + NZ, NZ),
            "ep_1": lax.rem(x + dx + NX, NX),
            "ep_2": lax.rem(c + dc + NC, NC),
            "tp": lax.rem(y + dy + NY, NY),
        }

    def send(src, dst, ss, rs, to):
        copy = pltpu.make_async_remote_copy(
            src_ref=src,
            dst_ref=dst,
            send_sem=ss,
            recv_sem=rs,
            device_id=to,
            device_id_type=pl.DeviceIdType.MESH,
        )
        copy.start()
        pending.append(copy)

    def arrive(dst, ss, rs):
        pltpu.make_async_remote_copy(
            src_ref=dst,
            dst_ref=dst,
            send_sem=ss,
            recv_sem=rs,
            device_id=dev(),
            device_id_type=pl.DeviceIdType.MESH,
        ).wait_recv()

    def zi(d):
        return lax.rem(z + d + NZ, NZ)

    def yi(d):
        return lax.rem(y + d + NY, NY)

    groups = [(dx, dc) for dx in range(NX) for dc in range(NC)]

    def xc_to(g):
        return lax.rem(x + g[0], NX) * NC + lax.rem(c + g[1], NC)

    def xc_from(g):
        return lax.rem(x - g[0] + NX, NX) * NC + lax.rem(c - g[1] + NC, NC)

    loads = [
        pltpu.make_async_copy(state_hbm, state_v, local.at[0]),
        pltpu.make_async_copy(eg_hbm, wg_v, local.at[1]),
        pltpu.make_async_copy(eu_hbm, wu_v, local.at[2]),
    ]
    early = [
        (wq_hbm, w_v.at[0]),
        (wf_hbm, w_v.at[1]),
        (wi_hbm, w_v.at[2]),
        (wg_hbm, w_v.at[3]),
        (wo_hbm, w_v.at[4]),
        (res_hbm, res_ref),
        (mix_gain_hbm, mix_gain_v),
        (lower_hbm, lower_v),
        (head_gain_hbm, head_gain_v),
        (ffn_gain_hbm, ffn_gain_v),
        (ids_hbm, ids_v),
        (rw_hbm, rw_v),
    ]
    early = [
        pltpu.make_async_copy(src, dst, local.at[8 + n])
        for n, (src, dst) in enumerate(early)
    ]
    for copy in early:
        copy.start()

    def quarter(ref, part):
        return ref.at[:, pl.ds(pl.multiple_of(part * Q, Q), Q)]

    own_down = pltpu.make_async_copy(quarter(ed_hbm, y), dq.at[y], local.at[3])

    barrier = pltpu.get_barrier_semaphore()
    peers = [dict(dz=d) for d in (1, -1, 4, -4)]
    for g in groups:
        for dy in range(NY):
            if g != (0, 0) or dy:
                peers.append(dict(dx=g[0], dc=g[1], dy=dy))
    for p in peers:
        pl.semaphore_signal(
            barrier, inc=1, device_id=dev(**p), device_id_type=pl.DeviceIdType.MESH
        )

    res_s[...] = jnp.zeros_like(res_s)
    w_all[...] = jnp.zeros_like(w_all)
    for copy in early:
        copy.wait()
    for n in range(5):
        w_all[n * COLS : (n + 1) * COLS, :] = w_v[n].astype(F32)
    wz[:, 48:64, :] = jnp.zeros((NZ, 16, Q), BF)
    wz[z, 0:48, :] = w_all[0:48, :].astype(BF)
    res_s[0:SEQ, :] = res_ref[...].astype(F32)
    res = res_s[...]
    mix_gain = mix_gain_v[pl.ds(pl.multiple_of(y * Q, Q), Q)].reshape(1, Q)
    ffn_gain = ffn_gain_v[pl.ds(pl.multiple_of(y * Q, Q), Q)].reshape(1, Q)
    lower_all = lower_v[...].reshape(1, Q)
    head_gain = head_gain_v[...].reshape(1, HEAD)
    scale = lax.rsqrt(jnp.mean(res * res, axis=-1, keepdims=True) + EPS)
    own = pl.ds(pl.multiple_of(y * Q, Q), Q)
    tok[me] = (res_s[:, own] * scale * mix_gain).astype(BF)
    pl.semaphore_wait(barrier, len(peers))

    def z_ways(view, ss, rs):
        def pass_on(k, d, to, half=None):
            send(view(d, half), view(d, half), ss.at[k], rs.at[k], dev(dz=to))

        def got(k, d, half=None):
            arrive(view(d, half), ss.at[k], rs.at[k])

        return pass_on, got

    def lean_start(ways):
        pass_on, _ = ways
        for k, to in ((2, 4), (3, -4), (0, 1), (1, -1)):
            pass_on(k, 0, to)

    def lean_middle(ways):
        pass_on, got = ways
        got(0, -1)
        pass_on(4, -1, 1)
        got(1, 1)
        pass_on(5, 1, -1)
        got(2, -4)
        pass_on(6, -4, 4, 0)
        got(3, 4)
        pass_on(10, 4, -4, 1)
        for k, d, to in ((7, -4, 1), (12, 4, -1), (8, -4, -1), (11, 4, 1)):
            pass_on(k, d, to)
        got(7, -5)
        pass_on(9, -5, 1)
        got(12, 5)
        pass_on(13, 5, -1)

    def lean_last(ways):
        pass_on, got = ways
        got(6, 8, 0)
        got(10, 8, 1)
        pass_on(14, 8, 1)
        pass_on(15, 8, -1)

    def lean_rest(ways):
        _, got = ways
        for k, d in ((4, -2), (5, 2), (8, -3), (9, -6), (11, 3), (13, 6), (14, 7), (15, 9)):
            got(k, d)

    def quick_start(ways):
        pass_on, _ = ways
        for k, to in ((6, 6), (7, -6), (4, 4), (5, -4), (2, 2), (3, -2), (0, 1), (1, -1)):
            pass_on(k, 0, to)

    def quick_middle(ways):
        pass_on, got = ways
        got(4, -4)
        pass_on(8, -4, -1)
        got(5, 4)
        pass_on(9, 4, 1)
        got(6, -6)
        pass_on(10, -6, 2, 0)
        pass_on(12, -6, 1)
        pass_on(13, -6, -1)
        got(7, 6)
        pass_on(11, 6, -2, 1)
        pass_on(14, 6, -1)
        pass_on(15, 6, 1)

    def quick_rest(ways):
        _, got = ways
        for k, d in ((0, -1), (1, 1), (2, -2), (3, 2), (8, -3), (9, 3), (12, -7), (13, -5), (14, 7), (15, 5)):
            got(k, d)
        got(10, 8, 0)
        got(11, 8, 1)

    def lanes_of(buf):
        def view(d, half):
            ref = buf.at[zi(d)]
            if half is None:
                return ref
            return ref.at[:, pl.ds(0, 256)] if half == 0 else ref.at[:, pl.ds(256, 128)]

        return view

    def rows_of(d, half):
        first, count = ((0, 48), (0, 32), (32, 16))[0 if half is None else half + 1]
        return wz.at[zi(d), pl.ds(first, count)]

    in_ways = z_ways(rows_of, z1s, z1r)
    out_ways = z_ways(lanes_of(wo), z3s, z3r)
    tok_ways = z_ways(lanes_of(tz), z2s, z2r)
    lean_start(in_ways)
    for i, g in enumerate(groups[1:], 1):
        send(tok.at[me], tok.at[me], toks.at[i], tokr.at[i], dev(dx=g[0], dc=g[1]))
    for copy in loads:
        copy.start()
    own_down.start()
    for k in range(1, NY):
        send(quarter(ed_hbm, yi(k)), dq.at[y], ds_.at[k], dr.at[k], dev(dy=k))

    ids_s[...] = jnp.full_like(ids_s, -1.0)
    ids_s[0:TOPK, 0:SEQ] = ids_v[...].astype(F32)
    rw_s[...] = jnp.zeros_like(rw_s)
    rw_s[0:TOPK, 0:SEQ] = rw_v[...]
    ids, rw = jnp.transpose(ids_s[...])[0:16], jnp.transpose(rw_s[...])[0:16]
    lane = iota((16, 256), 1)
    expert, slot = (lane // 2).astype(F32), lane % 2
    row = iota((16, 256), 0).astype(F32)
    named = jnp.zeros((16, 256), F32)
    weight = jnp.zeros((16, 256), F32)
    for j in range(TOPK):
        hit = ids[:, j : j + 1] == expert
        named = jnp.where(hit, 1.0, named)
        weight = jnp.where(hit, rw[:, j : j + 1], weight)
    low = jnp.min(jnp.where(named > 0.5, row, 99.0), axis=0, keepdims=True)
    high = jnp.max(jnp.where(named > 0.5, row, -1.0), axis=0, keepdims=True)
    second = jnp.where(high > low, high, 99.0)
    table = jnp.where(slot[0:1] == 0, low, second)
    combine = jnp.where(row == table, weight, 0.0)
    comb_hi, comb_lo = split_two(combine)

    table_row = jnp.concatenate([table, jnp.zeros((1, 128), F32)], axis=1)
    wo[z] = jnp.where(iota((16, Q), 0) == COLS, table_row, w_all[48:64, :]).astype(BF)

    k_id = iota((1024, 1), 0)
    k_xc, k_in = k_id // 128, k_id % 128
    k_q, k_pj = k_in // 64, k_in % 64
    k_p, k_j = k_pj // COLS, k_pj % COLS
    target = jnp.where(k_pj < 48, k_p * 256 + k_q * 96 + COLS * k_xc + k_j, -1)
    order_in = jnp.where(iota((1024, 1024), 1) == target, 1.0, 0.0).astype(BF)
    perm_in[...] = order_in
    o_id = iota((1024, 1), 0)
    o_xc, o_half, o_q, o_j = o_id // 128, (o_id // 64) % 2, (o_id // 16) % 4, o_id % 16
    o_ok = (o_j < COLS) & (o_half == lax.rem(y, 2))
    o_to = jnp.where(o_ok, 96 * o_q + COLS * o_xc + o_j, -1)
    order_out[...] = jnp.where(iota((1024, Q), 1) == o_to, 1.0, 0.0).astype(BF)

    home = res_s[...].astype(BF)
    f_id, l_one = iota((D, 1), 0), iota((D, 256), 1)
    for e in range(XC):
        f_in = f_id % 96 - COLS * e
        f_to = jnp.where((f_in >= 0) & (f_in < COLS), 16 * (f_id // 96) + f_in, -1)
        res_p[e] = dot(home, jnp.where(l_one == f_to, 1.0, 0.0).astype(BF))

    lean_middle(in_ways)
    lean_last(in_ways)
    quick_start(out_ways)
    lean_rest(in_ways)

    for i, g in enumerate(groups[1:], 1):
        arrive(tok.at[xc_from(g)], toks.at[i], tokr.at[i])
    tokens = tok[...].reshape(XC * 16, Q)

    pairs = [(g, dy) for dy in range(NY) for g in groups]
    for k in range(NY):
        part = yi(k)
        block = wz[pl.ds(4 * part, 4)].reshape(256, Q)
        psend[part] = dot_t(tokens, block).astype(BF).reshape(XC, 16, 256)
    precv[y, me] = psend[y, me]
    for i, (g, dy) in enumerate(pairs):
        if i == 0:
            continue
        send(
            psend.at[yi(dy), xc_to(g)],
            precv.at[y, me],
            ps.at[i],
            pr.at[i],
            dev(dx=g[0], dc=g[1], dy=dy),
        )
    for i, (g, dy) in enumerate(pairs):
        if i:
            arrive(precv.at[yi(-dy), xc_from(g)], ps.at[i], pr.at[i])
    quick_middle(out_ways)
    halves = [[], []]
    for e in range(XC):
        total = precv[0, e].astype(F32)
        for k in range(1, NY):
            total = total + precv[k, e].astype(F32)
        total = total.astype(BF)
        halves[0].append(total[:, 0:128])
        halves[1].append(total[:, 128:256])
    stacked = jnp.concatenate(
        [jnp.concatenate(half, axis=1) for half in halves], axis=0
    )
    ordered = dot(stacked, perm_in[...])
    narrow = iota((16, 128), 1) < 64
    proj = []
    for p in range(4):
        a = ordered[0:16, 256 * p : 256 * p + 256]
        b = ordered[16:32, 256 * p : 256 * p + 256]
        b0 = pltpu.roll(b[:, 0:128], 64, 1)
        b1 = pltpu.roll(b[:, 128:256], 64, 1)
        proj.append(
            [a[:, 0:128], jnp.where(narrow, a[:, 128:256], b0), jnp.where(narrow, b0, b1)]
        )
    gates = []
    for h in range(HL):
        lower = lower_all[:, h * HEAD : (h + 1) * HEAD]
        query = proj[0][h] * sigmoid(proj[0][h])
        forget = lower + (1.0 - lower) * sigmoid(proj[1][h])
        for n, values in enumerate((query, forget)):
            tall = jnp.concatenate([values, jnp.zeros((112, 128), F32)], axis=0)
            cols[n, h] = jnp.transpose(tall)
        rows_s[h] = proj[2][h]
        gates.append(proj[3][h] * sigmoid(proj[3][h]))

    loads[0].wait()
    read_s[...] = jnp.zeros_like(read_s)

    def one_head(h, _):
        queries, forgets, values = cols[0, h], cols[1, h], rows_s[h]
        for s in range(SEQ):
            f = forgets[:, s : s + 1]
            q = queries[:, s : s + 1]
            v = values[s : s + 1, :]
            nxt = f * state_v[s, h].astype(F32) + (1.0 - f) * v
            state_o[s, h] = nxt.astype(BF)
            read_s[h, s : s + 1, :] = jnp.sum(q * nxt, axis=0, keepdims=True)
        return 0

    lax.fori_loop(0, HL, one_head, 0)
    store = pltpu.make_async_copy(state_o, new_state_hbm, local.at[6])
    store.start()
    for h in range(HL):
        r = read_s[h]
        r = r * lax.rsqrt(jnp.mean(r * r, axis=-1, keepdims=True) + EPS)
        ho[:, h * HEAD : (h + 1) * HEAD] = (r * head_gain * gates[h]).astype(BF)

    hall[me] = ho[...]
    for i, g in enumerate(groups[1:], 1):
        send(hall.at[me], hall.at[me], hgs.at[i], hgr.at[i], dev(dx=g[0], dc=g[1]))
    quick_rest(out_ways)
    for i, g in enumerate(groups[1:], 1):
        arrive(hall.at[xc_from(g)], hgs.at[i], hgr.at[i])
    mixed = dot_t(hall[...].reshape(128, Q), wo[...].reshape(256, Q)).astype(BF)
    rsend[...] = mixed.reshape(XC, 16, 256)
    rrecv[y, me] = rsend[me]
    for i, (g, dy) in enumerate(pairs):
        if i:
            send(
                rsend.at[xc_to(g)],
                rrecv.at[y, me],
                rss.at[i],
                rsr.at[i],
                dev(dx=g[0], dc=g[1], dy=dy),
            )
    for i, (g, dy) in enumerate(pairs):
        if i:
            arrive(rrecv.at[yi(-dy), xc_from(g)], rss.at[i], rsr.at[i])
    squares = jnp.zeros((16, 256), F32)
    padding = iota((16, 256), 1) % 16 >= COLS
    for e in range(XC):
        total = rrecv[0, e].astype(F32)
        for k in range(1, NY):
            total = total + rrecv[k, e].astype(F32)
        total = jnp.where(padding, 0.0, total)
        after = (res_p[e] + total).astype(BF).astype(F32)
        squares = squares + after * after
        sum_s[e] = total
    square = jnp.sum(squares, axis=-1, keepdims=True)
    half = pl.ds(pl.multiple_of(128 * (y // 2), 128), 128)
    total = jnp.concatenate([sum_s[e, :, half] for e in range(XC)], axis=1)
    both = dot(jnp.concatenate(split_two(total), axis=0), order_out[...])
    after = (res_s[:, own] + (both[0:16] + both[16:32])).astype(BF).astype(F32)
    gained = after * ffn_gain
    inverse = lax.rsqrt(square * (1.0 / D) + EPS)
    tz[z] = (gained * inverse).astype(BF)

    quick_start(tok_ways)
    r_id, l_id = iota((256, 256), 0), iota((256, 256), 1)
    spread = jnp.where((r_id // 16 == l_id // 16) & (l_id % 16 == COLS), 1.0, 0.0).astype(BF)
    mine = jnp.where(iota((16, 256), 1) == 16 * z + iota((16, 256), 0), 1.0, 0.0).astype(BF)
    same = iota((16, 256), 0) == iota((16, 256), 1) // 16
    token = (iota((16, 256), 1) % 16).astype(F32)
    loads[1].wait()
    loads[2].wait()
    tables = dot(spread, wo[...].reshape(256, Q)[:, 0:256]).astype(BF)
    wanted = dot_t(mine, tables)
    hit = jnp.where(wanted == token, 1.0, 0.0)
    same_f = jnp.where(same, 1.0, 0.0)
    pick = (hit[:, None, :] * same_f[None, :, :]).reshape(256, 256).astype(BF)
    quick_middle(tok_ways)
    quick_rest(tok_ways)
    flat = tz[...].reshape(256, Q)
    xsend[...] = dot(pick, flat).astype(BF).reshape(XC, 32, Q)
    xf[y, me] = xsend[me]
    for i, g in enumerate(groups[1:], 1):
        send(xsend.at[xc_to(g)], xf.at[y, me], xs.at[i], xr.at[i], dev(dx=g[0], dc=g[1]))
    for i, g in enumerate(groups):
        chunk = xf.at[y, xc_from(g)]
        if i:
            arrive(chunk, xs.at[i], xr.at[i])
        send(chunk, chunk, ys.at[0, i], yr.at[0, i], dev(dy=1))
        send(chunk, chunk, ys.at[1, i], yr.at[1, i], dev(dy=-1))

    def weights_of(part):
        at = pl.ds(pl.multiple_of(part * Q, Q), Q)
        return wg_v[at, :], wu_v[at, :]

    def add_part(part, sums):
        rows = xf[part].reshape(256, Q)
        a, b = weights_of(part)
        return sums[0] + dot(rows, a), sums[1] + dot(rows, b)

    sums = add_part(y, (jnp.zeros((256, FQ), F32), jnp.zeros((256, FQ), F32)))
    for i, g in enumerate(groups):
        left = xf.at[yi(-1), xc_from(g)]
        right = xf.at[yi(1), xc_from(g)]
        arrive(left, ys.at[0, i], yr.at[0, i])
        if i < 4:
            send(left, left, ys.at[2, i], yr.at[2, i], dev(dy=1))
        arrive(right, ys.at[1, i], yr.at[1, i])
        if i >= 4:
            send(right, right, ys.at[2, i], yr.at[2, i], dev(dy=-1))
    sums = add_part(yi(-1), sums)
    sums = add_part(yi(1), sums)
    for i, g in enumerate(groups):
        arrive(xf.at[yi(2), xc_from(g)], ys.at[2, i], yr.at[2, i])
    gate, up = add_part(yi(2), sums)
    hf[y] = (gate * sigmoid(gate) * up).astype(BF)

    send(hf.at[y], hf.at[y], hs.at[0], hr.at[0], dev(dy=1))
    send(hf.at[y], hf.at[y], hs.at[1], hr.at[1], dev(dy=-1))
    send(hf.at[y, pl.ds(0, 128)], hf.at[y, pl.ds(0, 128)], hs.at[2], hr.at[2], dev(dy=2))
    send(hf.at[y, pl.ds(128, 128)], hf.at[y, pl.ds(128, 128)], hs.at[3], hr.at[3], dev(dy=-2))
    own_down.wait()
    for k in range(1, NY):
        arrive(dq.at[yi(-k)], ds_.at[k], dr.at[k])
    down = dot(hf[y], dq[y])
    top, bottom = pl.ds(0, 128), pl.ds(128, 128)
    left = hf.at[yi(-1)]
    right = hf.at[yi(1)]
    arrive(left, hs.at[0], hr.at[0])
    arrive(right, hs.at[1], hr.at[1])
    down = down + dot(hf[yi(-1)], dq[yi(-1)]) + dot(hf[yi(1)], dq[yi(1)])
    far = hf.at[yi(2)]
    arrive(far.at[top], hs.at[2], hr.at[2])
    arrive(far.at[bottom], hs.at[3], hr.at[3])
    down = down + dot(hf[yi(2)], dq[yi(2)])
    osend[...] = down.astype(BF).reshape(XC, 32, Q)

    orecv[me] = osend[me]
    parts = [pl.ds(0, Q)]
    for f, part in enumerate(parts):
        for i, g in enumerate(groups[1:], 1):
            send(
                osend.at[xc_to(g), :, part],
                orecv.at[me, :, part],
                os_.at[f, i],
                or_.at[f, i],
                dev(dx=g[0], dc=g[1]),
            )
    to_z, to_e = r_id // 16, r_id % 16
    source = (to_e // 2) * 32 + (to_e % 2) * 16 + to_z
    turn = jnp.where(l_id == source, 1.0, 0.0).astype(BF)
    for f, part in enumerate(parts):
        for i, g in enumerate(groups[1:], 1):
            arrive(orecv.at[xc_from(g), :, part], os_.at[f, i], or_.at[f, i])
        turned = dot(turn, orecv[:, :, 0:Q].reshape(256, Q))
        zsend[:, :, 0:Q] = turned.astype(BF).reshape(NZ, 16, Q)
        for d in (8, 7, 9, 6, 10, 5, 11, 4, 12, 3, 13, 2, 14, 1, 15):
            send(
                zsend.at[zi(d), :, part],
                zrecv.at[z, :, part],
                rets.at[f, d],
                retr.at[f, d],
                dev(dz=d),
            )
    zrecv[z] = zsend[z]
    comb = jnp.concatenate([comb_hi, comb_lo], axis=0)
    for f, part in enumerate(parts):
        for d in range(1, NZ):
            arrive(zrecv.at[zi(-d), :, part], rets.at[f, d], retr.at[f, d])
        span = slice(0, Q)
        both = dot(comb, zrecv[:, :, span].reshape(256, Q))
        result = (after[:, span] + (both[0:16] + both[16:32])).astype(BF)
        out_ref[:, span] = result[0:SEQ, :]
    store.wait()
    for copy in pending:
        copy.wait_send()


def shards(
    residual_in,
    rec_state,
    mix_gain,
    w_query,
    w_forget,
    w_input,
    w_gate,
    lower_bound,
    head_gain,
    w_out,
    ffn_gain,
    route_ids,
    route_weight,
    expert_gate,
    expert_up,
    expert_down,
):
    vmem = pl.BlockSpec(memory_space=pltpu.VMEM)
    hbm = pl.BlockSpec(memory_space=pltpu.HBM)
    anywhere = pl.BlockSpec(memory_space=pl.ANY)
    dma = pltpu.SemaphoreType.DMA
    out = pl.pallas_call(
        kernel,
        out_shape=(
            pltpu.VMEM((SEQ, Q), BF),
            pltpu.VMEM(rec_state.shape, BF),
        ),
        in_specs=[hbm] * 16,
        out_specs=(vmem, anywhere),
        scratch_shapes=[
            pltpu.VMEM((SEQ, D), BF),
            pltpu.VMEM((5, COLS, Q), BF),
            pltpu.VMEM((64, Q), F32),
            pltpu.VMEM((D,), F32),
            pltpu.VMEM((Q,), F32),
            pltpu.VMEM((HEAD,), F32),
            pltpu.VMEM((D,), F32),
            pltpu.VMEM((TOPK, SEQ), jnp.int32),
            pltpu.VMEM((TOPK, SEQ), F32),
            pltpu.VMEM((NZ, 64, Q), BF),
            pltpu.VMEM((NZ, 16, Q), BF),
            pltpu.VMEM((XC, 16, Q), BF),
            pltpu.VMEM((XC, 16, Q), BF),
            pltpu.VMEM((1024, Q), BF),
            pltpu.VMEM((NY, XC, 16, 256), BF),
            pltpu.VMEM((NY, XC, 16, 256), BF),
            pltpu.VMEM((1024, 1024), BF),
            pltpu.VMEM((SEQ, HL, HEAD, HEAD), BF),
            pltpu.VMEM((SEQ, HL, HEAD, HEAD), BF),
            pltpu.VMEM((2, HL, HEAD, 128), F32),
            pltpu.VMEM((HL, 16, HEAD), F32),
            pltpu.VMEM((HL, 16, HEAD), F32),
            pltpu.VMEM((16, Q), BF),
            pltpu.VMEM((XC, 16, 256), BF),
            pltpu.VMEM((NY, XC, 16, 256), BF),
            pltpu.VMEM((XC, 16, 256), F32),
            pltpu.VMEM((XC, 16, 256), F32),
            pltpu.VMEM((16, D), F32),
            pltpu.VMEM((128, 128), F32),
            pltpu.VMEM((128, 128), F32),
            pltpu.VMEM((NZ, 16, Q), BF),
            pltpu.VMEM((XC, 32, Q), BF),
            pltpu.VMEM((NY, XC, 32, Q), BF),
            pltpu.VMEM((NY, 256, FQ), BF),
            pltpu.VMEM((NY, FQ, Q), BF),
            pltpu.VMEM((D, FQ), BF),
            pltpu.VMEM((D, FQ), BF),
            pltpu.VMEM((XC, 32, Q), BF),
            pltpu.VMEM((XC, 32, Q), BF),
            pltpu.VMEM((NZ, 16, Q), BF),
            pltpu.VMEM((NZ, 16, Q), BF),
        ]
        + [
            dma((n,))
            for n in (16, 16, 8, 8, 32, 32, 8, 8, 16, 16, 32, 32, 16, 16, 8, 8)
        ]
        + [dma((3, 8)), dma((3, 8))]
        + [dma((n,)) for n in (4, 4, 4, 4)]
        + [dma((3, 8)), dma((3, 8)), dma((3, 16)), dma((3, 16)), dma((20,))],
        compiler_params=pltpu.CompilerParams(
            collective_id=0, has_side_effects=True, vmem_limit_bytes=60 * 1024 * 1024
        ),
    )(
        residual_in,
        w_query.T,
        w_forget.T,
        w_input.T,
        w_gate.T,
        w_out.T,
        mix_gain,
        lower_bound,
        head_gain,
        ffn_gain,
        route_ids.T,
        route_weight.T,
        rec_state,
        expert_gate.reshape(D, FQ),
        expert_up.reshape(D, FQ),
        expert_down.reshape(FQ, D),
    )
    return out


def solution(mesh):
    split = Mesh(mesh.devices.reshape(NZ, NX, NC, NY), ("ep_0", "ep_1", "ep_2", "tp"))
    in_specs = (
        P(EP, None),
        P(EP, "tp", None, None),
        P(),
        P("tp", EP),
        P("tp", EP),
        P("tp", EP),
        P("tp", EP),
        P("tp"),
        P(),
        P("tp", EP),
        P(),
        P(EP, None),
        P(EP, None),
        P(EP, None, "tp"),
        P(EP, None, "tp"),
        P(EP, "tp", None),
    )
    out_specs = (P(EP, "tp"), P(EP, "tp", None, None))
    return jax.shard_map(
        shards, mesh=split, in_specs=in_specs, out_specs=out_specs, check_vma=False
    )
```
